32 devices in a mesh: ep: 4 (over z), tp: 8 (over y, x, core).
Axes of the slice: x: 2, y: 2, z: 4, core: 2. Of those that a mesh axis runs over, the one named last changes fastest.
Arguments:
- tokens: bfloat16 [32, 4096], P('ep'), may hold values from -6 to 6
- norm_gains: float32 [4, 4096], replicated, may hold values from 0.1 to 1.9
- w_query: bfloat16 [4096, 4096], P(None, 'tp'), may hold values from -0.09375 to 0.09375
- w_query_rope: bfloat16 [4096, 2048], P(None, 'tp'), may hold values from -0.09375 to 0.09375
- w_key_up: bfloat16 [32, 128, 1024], P('tp'), may hold values from -0.5 to 0.5
- w_value_up: bfloat16 [32, 1024, 128], P('tp'), may hold values from -0.1875 to 0.1875
- w_output: bfloat16 [4096, 4096], P('tp'), may hold values from -0.09375 to 0.09375
- w_latent_down: bfloat16 [4096, 1024], P(None, 'tp'), may hold values from -0.09375 to 0.09375
- latent_gain: float32 [1024], replicated, may hold values from 0.1 to 1.9
- w_rope_down: bfloat16 [4096, 64], replicated, may hold values from -0.09375 to 0.09375
- cache_latent: bfloat16 [32, 1024, 1024], P(('ep', 'tp')), may hold values from -300 to 300
- cache_rope: bfloat16 [32, 1024, 64], P(('ep', 'tp')), may hold values from -6 to 6
- lengths: int32 [32], P(('ep', 'tp')), may hold values from 1 to 1024, as said below
- routes: int32 [32, 2], P('ep'), may hold values from 0 to 3, all different within a row; in each aligned block of 8 rows (0 to 7, 8 to 15, ...) at most 7 rows name the same one
- route_weights: float32 [32, 2], P('ep'), may hold values from 0.2 to 1
- w_gate: bfloat16 [4, 4096, 2048], P('ep', None, 'tp'), may hold values from -0.09375 to 0.09375
- w_up: bfloat16 [4, 4096, 2048], P('ep', None, 'tp'), may hold values from -0.09375 to 0.09375
- w_down: bfloat16 [4, 2048, 4096], P('ep', 'tp'), may hold values from -0.125 to 0.125
Outputs:
- hidden_out: bfloat16 [32, 4096], P(('ep', 'tp'))
- new_latent: bfloat16 [32, 1024], P(('ep', 'tp'))
- new_rope: bfloat16 [32, 64], P(('ep', 'tp'))
The draws below stay inside these ranges and needn't reach their ends.
Inputs may be any that keep to these rules, and one draw needn't show every extreme that they name: `routes`: within each aligned block of 8 rows no expert is named by more than 7 rows, a bound that some block reaches; the 2 experts of a row differ. The new token stands at position lengths; some sequence has exactly 1024.
All inputs are finite; a program needn't handle non-finite values.
Results may differ from the reference program's by a relative error of at most 0.02.
Values may be sent and summed in bfloat16 or wider, within the bound.
No kernel may reach another device: no remote copies, remote signals or barrier semaphores. Data moves between devices by JAX's collectives and lax.ppermute only.
A program may use at most 64 MiB of HBM per device.

```python
import math
import jax
import jax.numpy as jnp
import numpy as np
from jax import lax

D = 4096
HEADS = 32
NOPE = 128
ROPE = 64
VDIM = 128
LATENT = 1024
FF = 2048
TOPK = 2
EXP_LOCAL = 1
CACHE = 1024
EXPERTS = 4
GROUP_ROWS = 8
TOKENS = 32
CAP = 7
FF_DEV = 256
N_EP = 4


def draw_cache_latent(key, part):
    base_key = jax.random.fold_in(jax.random.fold_in(key, 11), 0)
    drawn = jnp.clip(jax.random.normal(base_key, (TOKENS, CACHE, LATENT), jnp.float32), -6.0, 6.0)
    return drawn.astype(jnp.bfloat16)


def draw_lengths(key, part):
    value_key, place_key = jax.random.split(jax.random.fold_in(key, 13))
    drawn = jax.random.randint(value_key, (TOKENS,), 1, CACHE + 1)
    longest = jax.random.randint(place_key, (), 0, TOKENS)
    return jnp.where(jnp.arange(TOKENS) == longest, CACHE, drawn).astype(jnp.int32)


def block_levels(key, extent, cuts, least, high):
    gain = 1.0
    for dim, blocks in cuts:
        steps = jax.random.uniform(jax.random.fold_in(jax.random.fold_in(key, 6), dim), (blocks,), jnp.float32, least / len(cuts), high / len(cuts))
        gain = gain * jnp.repeat(jnp.exp(steps), extent[dim] // blocks).reshape((-1,) + (1,) * (len(extent) - 1 - dim))
    return gain


def shared_out(stream_key, own, number, rows, count, top, reach, lean):
    sequence = jax.random.permutation(stream_key, count)
    crowded, ordinary = load_shares(count, rows * top, reach, lean, True), load_shares(count, rows * top, reach, lean, False)
    places = jnp.arange(count)

    def named(sizes, rotation):
        used = int((sizes > 0).sum())
        fixed = max(1, used // 4)
        shifted = fixed + (places - fixed + rotation * (used - fixed)) % max(1, count - fixed)
        return jnp.zeros((count,), jnp.int32).at[sequence[jnp.where(places < fixed, places, shifted)]].set(jnp.asarray(sizes, jnp.int32))

    sizes = jnp.where(number % 4 == 0, named(crowded, number // 4), named(ordinary, number - number // 4 - 1))
    mixed = jax.random.permutation(jax.random.fold_in(own, 3), count)
    source_of, receiver = mixed[0:count // 2 * 2:2], mixed[1:count // 2 * 2:2]
    slack = jnp.minimum(sizes[source_of] - 1, reach - sizes[receiver]) // 2
    slack = jnp.where((source_of == sequence[0]) | (receiver == sequence[0]) | (sizes[receiver] == 0), 0, jnp.maximum(slack, 0))
    shifted = jax.random.randint(jax.random.fold_in(own, 4), (count // 2,), 0, 1 << 20) % (slack + 1)
    sizes = sizes.at[source_of].add(-shifted).at[receiver].add(shifted)
    items = jnp.searchsorted(jnp.cumsum(sizes), jnp.arange(rows * top), side="right").astype(jnp.int32)
    table = items.reshape(top, rows).T
    table = table[jax.random.permutation(jax.random.fold_in(own, 1), rows)]
    rotation = jax.random.randint(jax.random.fold_in(own, 2), (rows, 1), 0, top)
    return jnp.take_along_axis(table, (jnp.arange(top)[None, :] + rotation) % top, axis=1)


def load_shares(number_of, total, bound, skew, full):
    loads = [(1 << 20) // math.isqrt(grade ** skew) + 1 for grade in range(1, number_of + 1)]
    largest = bound if full else min(bound, max(-(-total // number_of), total * loads[0] // sum(loads)))
    least = 1 if total - largest >= number_of - 1 else 0
    counts, rest = [largest] + [least] * (number_of - 1), total - largest - least * (number_of - 1)
    while rest > 0:
        movable = [i for i in range(1, number_of) if counts[i] < largest] or [i for i in range(1, number_of) if counts[i] < bound]
        mass, remaining = sum([loads[i] for i in movable]), rest
        for i in movable:
            addition = min(bound - counts[i], max(1, remaining * loads[i] // mass), rest)
            counts[i] = counts[i] + addition
            rest = rest - addition
    return np.array(counts)


def normal_values(stream_key, shape, scale, bound, pieces=(), kind=jnp.bfloat16):
    values = jax.random.normal(stream_key, shape, jnp.float32) * scale
    if len(pieces) > 0:
        values = block_levels(stream_key, shape, pieces, -0.22, 0.18) * values
    return jnp.clip(values, min=-bound, max=bound).astype(kind)


def setup_inputs(seed: int = 0) -> dict:
    seeds = jax.random.split(jax.random.key(seed), 19)
    tokens = normal_values(seeds[0], (TOKENS, D), 1.0, 6.0, ((0, 4),))
    norm_gains = jnp.clip(1.0 + 0.18 * jax.random.normal(seeds[1], (4, D), jnp.float32), 0.1, 1.9)
    w_query = normal_values(seeds[2], (D, HEADS * NOPE), D ** -0.5, 0.09375, ((1, 8),))
    w_query_rope = normal_values(seeds[3], (D, HEADS * ROPE), D ** -0.5, 0.09375, ((1, 8),))
    w_key_up = normal_values(seeds[4], (HEADS, NOPE, LATENT), NOPE ** -0.5, 0.5, ((0, 8),))
    w_value_up = normal_values(seeds[5], (HEADS, LATENT, VDIM), LATENT ** -0.5, 0.1875, ((0, 8),))
    w_output = normal_values(seeds[6], (HEADS * VDIM, D), (HEADS * VDIM) ** -0.5, 0.09375, ((0, 8),))
    w_latent_down = normal_values(seeds[7], (D, LATENT), D ** -0.5, 0.09375, ((1, 8),))
    latent_gain = jnp.clip(1.0 + 0.18 * jax.random.normal(seeds[8], (LATENT,), jnp.float32), 0.1, 1.9)
    w_rope_down = normal_values(seeds[9], (D, ROPE), D ** -0.5, 0.09375)
    cache_latent = draw_cache_latent(jax.random.fold_in(seeds[18], 71), 0)
    cache_rope = normal_values(seeds[11], (TOKENS, CACHE, ROPE), 1.0, 6.0, ((0, 32),))
    lengths = draw_lengths(jax.random.fold_in(seeds[18], 71), 0)
    routes_keys = jax.random.split(jax.random.fold_in(seeds[13], 1), TOKENS // GROUP_ROWS)
    routes_turns = jax.random.permutation(jax.random.fold_in(seeds[13], 3), TOKENS // GROUP_ROWS)
    routes = jax.vmap(lambda own, number: shared_out(jax.random.fold_in(seeds[13], 2), own, number, GROUP_ROWS, EXPERTS, TOPK, CAP, 2))(routes_keys, routes_turns).reshape((TOKENS, TOPK))
    route_weights = jnp.clip(0.2 + 0.8 * jax.random.uniform(seeds[14], (TOKENS, TOPK), jnp.float32) ** block_levels(seeds[14], (TOKENS, TOPK), ((0, 4),), -0.2, 0.2), 0.2, 1.0)
    w_gate = normal_values(seeds[15], (EXPERTS // EXP_LOCAL, D, EXP_LOCAL * FF), D ** -0.5, 0.09375, ((0, 4), (2, 8)))
    w_up = normal_values(seeds[16], (EXPERTS // EXP_LOCAL, D, EXP_LOCAL * FF), D ** -0.5, 0.09375, ((0, 4), (2, 8)))
    w_down = normal_values(seeds[17], (EXPERTS // EXP_LOCAL, EXP_LOCAL * FF, D), FF ** -0.5, 0.125, ((0, 4), (1, 8)))
    return dict(tokens=tokens, norm_gains=norm_gains, w_query=w_query, w_query_rope=w_query_rope, w_key_up=w_key_up, w_value_up=w_value_up, w_output=w_output, w_latent_down=w_latent_down, latent_gain=latent_gain, w_rope_down=w_rope_down, cache_latent=cache_latent, cache_rope=cache_rope, lengths=lengths, routes=routes, route_weights=route_weights, w_gate=w_gate, w_up=w_up, w_down=w_down)


EPSILON = 1e-06
ROTARY_BASE = 500000.0

def rms_scale(source, gain_row):
    values_f = source.astype(jnp.float32)
    return values_f * lax.rsqrt(lax.optimization_barrier(jnp.mean(values_f * values_f, axis=-1, keepdims=True)) + EPSILON) * gain_row.astype(jnp.float32)

def rotate(source, position):
    half_width = source.shape[-1] // 2
    frequency = ROTARY_BASE ** (-jnp.arange(half_width, dtype=jnp.float32) / half_width)
    angles = position[..., None] * frequency
    first_half = source[..., :half_width]
    second_half = source[..., half_width:]
    return jnp.concatenate([first_half * jnp.cos(angles) - second_half * jnp.sin(angles), second_half * jnp.cos(angles) + first_half * jnp.sin(angles)], axis=-1)

def attend_one(items):
    q_latent, q_pe, cache_lat, cache_rp, lat_new, rope_new, length = items
    score_scale = (NOPE + ROPE) ** (-0.5)
    scores = (jnp.einsum('hc,pc->hp', q_latent.astype(jnp.float32), cache_lat.astype(jnp.float32)) + jnp.einsum('hr,pr->hp', q_pe.astype(jnp.float32), cache_rp.astype(jnp.float32))) * score_scale
    own_score = (jnp.einsum('hc,c->h', q_latent.astype(jnp.float32), lat_new.astype(jnp.float32)) + jnp.einsum('hr,r->h', q_pe.astype(jnp.float32), rope_new.astype(jnp.float32))) * score_scale
    visible = (jnp.arange(CACHE, dtype=jnp.int32) < length)[None, :]
    row_max = jnp.maximum(lax.optimization_barrier(jnp.max(jnp.where(visible, scores, -jnp.inf), axis=-1)), own_score)
    weights = jnp.where(visible, jnp.exp(scores - row_max[:, None]), 0.0)
    own_weight = jnp.exp(own_score - row_max)
    denominator = lax.optimization_barrier(jnp.sum(weights, axis=-1)) + own_weight
    probabilities = (weights / denominator[:, None]).astype(jnp.bfloat16)
    own_prob = (own_weight / denominator).astype(jnp.bfloat16)
    attended = jnp.einsum('hp,pc->hc', probabilities.astype(jnp.float32), cache_lat.astype(jnp.float32))
    attended = attended + own_prob.astype(jnp.float32)[:, None] * lat_new.astype(jnp.float32)[None, :]
    return attended.astype(jnp.bfloat16)

def expert_total(expert_in, routes, route_weights, w_gate, w_up, w_down):
    slot_count = N_EP * CAP
    block_count = FF // FF_DEV

    def one_expert(running, expert):
        holder = (expert // EXP_LOCAL).astype(jnp.int32)
        offset = (expert % EXP_LOCAL * FF).astype(jnp.int32)
        gate_cols = lax.dynamic_slice_in_dim(w_gate[holder], offset, FF, 1)
        up_cols = lax.dynamic_slice_in_dim(w_up[holder], offset, FF, 1)
        down_rows = lax.dynamic_slice_in_dim(w_down[holder], offset, FF, 0)
        hit_mask = routes == expert
        chosen = jnp.any(hit_mask, axis=-1)
        route_weight = lax.optimization_barrier(jnp.sum(jnp.where(hit_mask, route_weights, 0.0), axis=-1))
        slot_place = (jnp.cumsum(chosen.astype(jnp.int32)) - 1).astype(jnp.int32)
        slot_target = jnp.where(chosen, slot_place, slot_count).astype(jnp.int32)
        row_index = jnp.zeros((slot_count,), jnp.int32).at[slot_target].set(jnp.arange(TOKENS, dtype=jnp.int32), mode='drop')
        expert_rows = expert_in[row_index]
        gate_sum = jnp.dot(expert_rows, gate_cols, preferred_element_type=jnp.float32)
        up_sum = jnp.dot(expert_rows, up_cols, preferred_element_type=jnp.float32)
        hidden_units = (jax.nn.silu(gate_sum) * up_sum).astype(jnp.bfloat16)
        blocks = jnp.einsum('nbf,bfd->nbd', hidden_units.reshape(slot_count, block_count, FF_DEV).astype(jnp.float32), down_rows.reshape(block_count, FF_DEV, D).astype(jnp.float32)).astype(jnp.bfloat16)
        block_sum = lax.optimization_barrier(jnp.sum(blocks.astype(jnp.float32), axis=1))
        picked = block_sum[jnp.clip(slot_place, 0, slot_count - 1).astype(jnp.int32)]
        return (running + jnp.where(chosen[:, None], route_weight[:, None] * picked, 0.0), None)
    start = jnp.zeros((TOKENS, D), jnp.float32)
    return lax.scan(one_expert, start, jnp.arange(EXPERTS, dtype=jnp.int32))[0]

def reference(tokens, norm_gains, w_query, w_query_rope, w_key_up, w_value_up, w_output, w_latent_down, latent_gain, w_rope_down, cache_latent, cache_rope, lengths, routes, route_weights, w_gate, w_up, w_down):
    normed = rms_scale(tokens, norm_gains[0]).astype(jnp.bfloat16)
    q_nope = jnp.dot(normed, w_query, preferred_element_type=jnp.float32).astype(jnp.bfloat16).reshape(TOKENS, HEADS, NOPE)
    q_latent = jnp.einsum('thn,hnc->thc', q_nope.astype(jnp.float32), w_key_up.astype(jnp.float32)).astype(jnp.bfloat16)
    q_rot = jnp.dot(normed, w_query_rope, preferred_element_type=jnp.float32).astype(jnp.bfloat16).reshape(TOKENS, HEADS, ROPE)
    latent_raw = jnp.dot(normed, w_latent_down, preferred_element_type=jnp.float32).astype(jnp.bfloat16)
    rope_raw = jnp.dot(normed, w_rope_down, preferred_element_type=jnp.float32).astype(jnp.bfloat16)
    new_latent = rms_scale(latent_raw, latent_gain).astype(jnp.bfloat16)
    position = lengths.astype(jnp.float32)
    new_rope = rotate(rope_raw.astype(jnp.float32), position).astype(jnp.bfloat16)
    q_pe = rotate(q_rot.astype(jnp.float32), position[:, None]).astype(jnp.bfloat16)
    attended = lax.map(attend_one, (q_latent, q_pe, cache_latent, cache_rope, new_latent, new_rope, lengths))
    values = jnp.einsum('thc,hcv->thv', attended.astype(jnp.float32), w_value_up.astype(jnp.float32)).astype(jnp.bfloat16)
    mixed = jnp.dot(values.reshape(TOKENS, HEADS * VDIM), w_output, preferred_element_type=jnp.float32)
    resid = (tokens.astype(jnp.float32) + rms_scale(mixed, norm_gains[1])).astype(jnp.bfloat16)
    expert_in = rms_scale(resid, norm_gains[2]).astype(jnp.bfloat16)
    routed = expert_total(expert_in, routes, route_weights, w_gate, w_up, w_down)
    hidden_out = (resid.astype(jnp.float32) + rms_scale(routed, norm_gains[3])).astype(jnp.bfloat16)
    return (hidden_out, new_latent, new_rope)
```

```python
import jax
import jax.numpy as jnp
from jax import lax
from jax.sharding import PartitionSpec as P

EPSILON = 1e-06
ROTARY_BASE = 500000.0


def rms_scale(source, gain_row):
    values_f = source.astype(jnp.float32)
    return (
        values_f
        * lax.rsqrt(jnp.mean(values_f * values_f, axis=-1, keepdims=True) + EPSILON)
        * gain_row
    )


def rotate(source, position):
    half_width = source.shape[-1] // 2
    frequency = ROTARY_BASE ** (-jnp.arange(half_width, dtype=jnp.float32) / half_width)
    angles = position[..., None] * frequency
    first_half = source[..., :half_width]
    second_half = source[..., half_width:]
    return jnp.concatenate(
        [
            first_half * jnp.cos(angles) - second_half * jnp.sin(angles),
            second_half * jnp.cos(angles) + first_half * jnp.sin(angles),
        ],
        axis=-1,
    )


def attend(q_latent, q_pe, cache_lat, cache_rp, lat_new, rope_new, lengths, score_scale):
    scores = (
        jnp.einsum("shc,spc->shp", q_latent, cache_lat, preferred_element_type=jnp.float32)
        + jnp.einsum("shr,spr->shp", q_pe, cache_rp, preferred_element_type=jnp.float32)
    ) * score_scale
    own_score = (
        jnp.einsum("shc,sc->sh", q_latent, lat_new, preferred_element_type=jnp.float32)
        + jnp.einsum("shr,sr->sh", q_pe, rope_new, preferred_element_type=jnp.float32)
    ) * score_scale
    visible = (
        jnp.arange(cache_lat.shape[1], dtype=jnp.int32)[None, None, :] < lengths[:, None, None]
    )
    row_max = jnp.maximum(jnp.max(jnp.where(visible, scores, -jnp.inf), axis=-1), own_score)
    weights = jnp.where(visible, jnp.exp(scores - row_max[..., None]), 0.0)
    own_weight = jnp.exp(own_score - row_max)
    denominator = jnp.sum(weights, axis=-1) + own_weight
    probabilities = (weights / denominator[..., None]).astype(jnp.bfloat16)
    own_prob = (own_weight / denominator).astype(jnp.bfloat16)
    attended = jnp.einsum(
        "shp,spc->shc", probabilities, cache_lat, preferred_element_type=jnp.float32
    )
    attended = (
        attended + own_prob.astype(jnp.float32)[..., None] * lat_new.astype(jnp.float32)[:, None, :]
    )
    return attended.astype(jnp.bfloat16)


def to_sequences(rows, tp_size, seq_count):
    blocks = rows.reshape(tp_size, seq_count, rows.shape[1])
    return lax.all_to_all(blocks, "tp", split_axis=0, concat_axis=0, tiled=True)


def on_device(
    tokens,
    norm_gains,
    w_query,
    w_query_rope,
    w_key_up,
    w_value_up,
    w_output,
    w_latent_down,
    latent_gain,
    w_rope_down,
    cache_latent,
    cache_rope,
    lengths,
    routes,
    route_weights,
    w_gate,
    w_up,
    w_down,
):
    group_rows = tokens.shape[0]
    seq_count = cache_latent.shape[0]
    heads_here = w_key_up.shape[0]
    nope_width = w_key_up.shape[1]
    rope_width = w_rope_down.shape[1]
    tp_size = lax.axis_size("tp")
    tp_rank = lax.axis_index("tp")
    normed = rms_scale(tokens, norm_gains[0]).astype(jnp.bfloat16)
    q_nope = jnp.dot(normed, w_query, preferred_element_type=jnp.float32).astype(jnp.bfloat16)
    q_nope = q_nope.reshape(group_rows, heads_here, nope_width)
    q_latent = jnp.einsum("thn,hnc->thc", q_nope, w_key_up, preferred_element_type=jnp.float32)
    q_latent = q_latent.astype(jnp.bfloat16).reshape(group_rows, -1)
    q_rot = jnp.dot(normed, w_query_rope, preferred_element_type=jnp.float32).astype(jnp.bfloat16)
    latent_cols = jnp.dot(normed, w_latent_down, preferred_element_type=jnp.float32).astype(
        jnp.bfloat16
    )
    q_cols, rot_cols = q_latent.shape[1], q_rot.shape[1]
    packed = jnp.concatenate([q_latent, q_rot, latent_cols], axis=1)
    packed = to_sequences(packed, tp_size, seq_count)
    q_mine = packed[:, :, :q_cols].transpose(1, 0, 2).reshape(seq_count, -1)
    rot_mine = packed[:, :, q_cols : q_cols + rot_cols].transpose(1, 0, 2).reshape(seq_count, -1)
    latent_raw = packed[:, :, q_cols + rot_cols :].transpose(1, 0, 2).reshape(seq_count, -1)
    heads_all = rot_mine.shape[1] // rope_width
    own_normed = lax.dynamic_slice_in_dim(normed, tp_rank * seq_count, seq_count, 0)
    rope_raw = jnp.dot(own_normed, w_rope_down, preferred_element_type=jnp.float32).astype(
        jnp.bfloat16
    )
    new_latent = rms_scale(latent_raw, latent_gain).astype(jnp.bfloat16)
    position = lengths.astype(jnp.float32)
    new_rope = rotate(rope_raw.astype(jnp.float32), position).astype(jnp.bfloat16)
    q_pe = rotate(
        rot_mine.reshape(seq_count, heads_all, rope_width).astype(jnp.float32), position[:, None]
    )
    q_pe = q_pe.astype(jnp.bfloat16)
    score_scale = (nope_width + rope_width) ** (-0.5)
    attended = attend(
        q_mine.reshape(seq_count, heads_all, -1),
        q_pe,
        cache_latent,
        cache_rope,
        new_latent,
        new_rope,
        lengths,
        score_scale,
    )
    head_latent = lax.all_to_all(
        attended.reshape(seq_count, -1), "tp", split_axis=1, concat_axis=0, tiled=True
    )
    values = (
        jnp.einsum(
            "thc,hcv->thv",
            head_latent.reshape(group_rows, heads_here, -1),
            w_value_up,
            preferred_element_type=jnp.float32,
        )
        .astype(jnp.bfloat16)
        .reshape(group_rows, -1)
    )
    head_term = jnp.dot(values, w_output, preferred_element_type=jnp.float32)
    terms = to_sequences(head_term.astype(jnp.bfloat16), tp_size, seq_count)
    mixed = jnp.sum(terms.astype(jnp.float32), axis=0)
    own_tokens = lax.dynamic_slice_in_dim(tokens, tp_rank * seq_count, seq_count, 0)
    own_resid = (own_tokens.astype(jnp.float32) + rms_scale(mixed, norm_gains[1])).astype(
        jnp.bfloat16
    )
    expert_in = rms_scale(own_resid, norm_gains[2]).astype(jnp.bfloat16)
    everyone = ("ep", "tp")
    devices = lax.axis_size("ep") * tp_size
    copies = jnp.broadcast_to(expert_in[None], (devices,) + expert_in.shape)
    arrived = lax.all_to_all(copies, everyone, split_axis=0, concat_axis=0, tiled=True)
    arrived = arrived.reshape(devices * seq_count, -1)
    gate_sum = jnp.dot(arrived, w_gate[0], preferred_element_type=jnp.float32)
    up_sum = jnp.dot(arrived, w_up[0], preferred_element_type=jnp.float32)
    hidden_units = (jax.nn.silu(gate_sum) * up_sum).astype(jnp.bfloat16)
    pieces = jnp.dot(hidden_units, w_down[0], preferred_element_type=jnp.float32).astype(
        jnp.bfloat16
    )
    pieces = pieces.reshape(devices, seq_count, -1)
    returned = lax.all_to_all(pieces, everyone, split_axis=0, concat_axis=0, tiled=True)
    own_routes = lax.dynamic_slice_in_dim(routes, tp_rank * seq_count, seq_count, 0)
    own_weights = lax.dynamic_slice_in_dim(route_weights, tp_rank * seq_count, seq_count, 0)
    holder = jnp.arange(devices, dtype=jnp.int32) // tp_size
    picks = own_routes[None, :, :] == holder[:, None, None]
    scale = jnp.sum(jnp.where(picks, own_weights[None], 0.0), axis=-1)
    routed = jnp.sum(scale[:, :, None] * returned.astype(jnp.float32), axis=0)
    hidden_out = (own_resid.astype(jnp.float32) + rms_scale(routed, norm_gains[3])).astype(
        jnp.bfloat16
    )
    return (hidden_out, new_latent, new_rope)


def solution(mesh):
    in_specs = (
        P("ep", None),
        P(),
        P(None, "tp"),
        P(None, "tp"),
        P("tp", None, None),
        P("tp", None, None),
        P("tp", None),
        P(None, "tp"),
        P(),
        P(),
        P(("ep", "tp"), None, None),
        P(("ep", "tp"), None, None),
        P(("ep", "tp")),
        P("ep", None),
        P("ep", None),
        P("ep", None, "tp"),
        P("ep", None, "tp"),
        P("ep", "tp", None),
    )
    out_specs = (P(("ep", "tp"), None), P(("ep", "tp"), None), P(("ep", "tp"), None))
    return jax.shard_map(
        on_device, mesh=mesh, in_specs=in_specs, out_specs=out_specs, check_vma=False
    )
```

```python
import functools
import math

import jax
import jax.numpy as jnp
from jax import lax
from jax.experimental import pallas as pl
from jax.experimental.pallas import tpu as pltpu
from jax.sharding import PartitionSpec as P

EPSILON = 1e-06
ROTARY_BASE = 500000.0


def rms_scale(source, gain_row):
    values_f = source.astype(jnp.float32)
    return (
        values_f
        * lax.rsqrt(jnp.mean(values_f * values_f, axis=-1, keepdims=True) + EPSILON)
        * gain_row
    )


def rotate(source, position):
    half_width = source.shape[-1] // 2
    frequency = ROTARY_BASE ** (-jnp.arange(half_width, dtype=jnp.float32) / half_width)
    angles = position[..., None] * frequency
    first_half = source[..., :half_width]
    second_half = source[..., half_width:]
    return jnp.concatenate(
        [
            first_half * jnp.cos(angles) - second_half * jnp.sin(angles),
            second_half * jnp.cos(angles) + first_half * jnp.sin(angles),
        ],
        axis=-1,
    )


def attend(q_latent, q_pe, cache_lat, cache_rp, lat_new, rope_new, lengths, score_scale):
    scores = (
        jnp.einsum("shc,spc->shp", q_latent, cache_lat, preferred_element_type=jnp.float32)
        + jnp.einsum("shr,spr->shp", q_pe, cache_rp, preferred_element_type=jnp.float32)
    ) * score_scale
    own_score = (
        jnp.einsum("shc,sc->sh", q_latent, lat_new, preferred_element_type=jnp.float32)
        + jnp.einsum("shr,sr->sh", q_pe, rope_new, preferred_element_type=jnp.float32)
    ) * score_scale
    visible = (
        jnp.arange(cache_lat.shape[1], dtype=jnp.int32)[None, None, :] < lengths[:, None, None]
    )
    row_max = jnp.maximum(jnp.max(jnp.where(visible, scores, -jnp.inf), axis=-1), own_score)
    weights = jnp.where(visible, jnp.exp(scores - row_max[..., None]), 0.0)
    own_weight = jnp.exp(own_score - row_max)
    denominator = jnp.sum(weights, axis=-1) + own_weight
    probabilities = (weights / denominator[..., None]).astype(jnp.bfloat16)
    own_prob = (own_weight / denominator).astype(jnp.bfloat16)
    attended = jnp.einsum(
        "shp,spc->shc", probabilities, cache_lat, preferred_element_type=jnp.float32
    )
    attended = (
        attended + own_prob.astype(jnp.float32)[..., None] * lat_new.astype(jnp.float32)[:, None, :]
    )
    return attended.astype(jnp.bfloat16)


def to_sequences(rows, tp_size, seq_count):
    blocks = rows.reshape(tp_size, seq_count, rows.shape[1])
    return lax.all_to_all(blocks, "tp", split_axis=0, concat_axis=0, tiled=True)


def on_device_plain(
    tokens,
    norm_gains,
    w_query,
    w_query_rope,
    w_key_up,
    w_value_up,
    w_output,
    w_latent_down,
    latent_gain,
    w_rope_down,
    cache_latent,
    cache_rope,
    lengths,
    routes,
    route_weights,
    w_gate,
    w_up,
    w_down,
):
    group_rows = tokens.shape[0]
    seq_count = cache_latent.shape[0]
    heads_here = w_key_up.shape[0]
    nope_width = w_key_up.shape[1]
    rope_width = w_rope_down.shape[1]
    tp_size = lax.axis_size("tp")
    tp_rank = lax.axis_index("tp")
    normed = rms_scale(tokens, norm_gains[0]).astype(jnp.bfloat16)
    q_nope = jnp.dot(normed, w_query, preferred_element_type=jnp.float32).astype(jnp.bfloat16)
    q_nope = q_nope.reshape(group_rows, heads_here, nope_width)
    q_latent = jnp.einsum("thn,hnc->thc", q_nope, w_key_up, preferred_element_type=jnp.float32)
    q_latent = q_latent.astype(jnp.bfloat16).reshape(group_rows, -1)
    q_rot = jnp.dot(normed, w_query_rope, preferred_element_type=jnp.float32).astype(jnp.bfloat16)
    latent_cols = jnp.dot(normed, w_latent_down, preferred_element_type=jnp.float32).astype(
        jnp.bfloat16
    )
    q_cols, rot_cols = q_latent.shape[1], q_rot.shape[1]
    packed = jnp.concatenate([q_latent, q_rot, latent_cols], axis=1)
    packed = to_sequences(packed, tp_size, seq_count)
    q_mine = packed[:, :, :q_cols].transpose(1, 0, 2).reshape(seq_count, -1)
    rot_mine = packed[:, :, q_cols : q_cols + rot_cols].transpose(1, 0, 2).reshape(seq_count, -1)
    latent_raw = packed[:, :, q_cols + rot_cols :].transpose(1, 0, 2).reshape(seq_count, -1)
    heads_all = rot_mine.shape[1] // rope_width
    own_normed = lax.dynamic_slice_in_dim(normed, tp_rank * seq_count, seq_count, 0)
    rope_raw = jnp.dot(own_normed, w_rope_down, preferred_element_type=jnp.float32).astype(
        jnp.bfloat16
    )
    new_latent = rms_scale(latent_raw, latent_gain).astype(jnp.bfloat16)
    position = lengths.astype(jnp.float32)
    new_rope = rotate(rope_raw.astype(jnp.float32), position).astype(jnp.bfloat16)
    q_pe = rotate(
        rot_mine.reshape(seq_count, heads_all, rope_width).astype(jnp.float32), position[:, None]
    )
    q_pe = q_pe.astype(jnp.bfloat16)
    score_scale = (nope_width + rope_width) ** (-0.5)
    attended = attend(
        q_mine.reshape(seq_count, heads_all, -1),
        q_pe,
        cache_latent,
        cache_rope,
        new_latent,
        new_rope,
        lengths,
        score_scale,
    )
    head_latent = lax.all_to_all(
        attended.reshape(seq_count, -1), "tp", split_axis=1, concat_axis=0, tiled=True
    )
    values = (
        jnp.einsum(
            "thc,hcv->thv",
            head_latent.reshape(group_rows, heads_here, -1),
            w_value_up,
            preferred_element_type=jnp.float32,
        )
        .astype(jnp.bfloat16)
        .reshape(group_rows, -1)
    )
    head_term = jnp.dot(values, w_output, preferred_element_type=jnp.float32)
    terms = to_sequences(head_term.astype(jnp.bfloat16), tp_size, seq_count)
    mixed = jnp.sum(terms.astype(jnp.float32), axis=0)
    own_tokens = lax.dynamic_slice_in_dim(tokens, tp_rank * seq_count, seq_count, 0)
    own_resid = (own_tokens.astype(jnp.float32) + rms_scale(mixed, norm_gains[1])).astype(
        jnp.bfloat16
    )
    expert_in = rms_scale(own_resid, norm_gains[2]).astype(jnp.bfloat16)
    everyone = ("ep", "tp")
    devices = lax.axis_size("ep") * tp_size
    copies = jnp.broadcast_to(expert_in[None], (devices,) + expert_in.shape)
    arrived = lax.all_to_all(copies, everyone, split_axis=0, concat_axis=0, tiled=True)
    arrived = arrived.reshape(devices * seq_count, -1)
    gate_sum = jnp.dot(arrived, w_gate[0], preferred_element_type=jnp.float32)
    up_sum = jnp.dot(arrived, w_up[0], preferred_element_type=jnp.float32)
    hidden_units = (jax.nn.silu(gate_sum) * up_sum).astype(jnp.bfloat16)
    pieces = jnp.dot(hidden_units, w_down[0], preferred_element_type=jnp.float32).astype(
        jnp.bfloat16
    )
    pieces = pieces.reshape(devices, seq_count, -1)
    returned = lax.all_to_all(pieces, everyone, split_axis=0, concat_axis=0, tiled=True)
    own_routes = lax.dynamic_slice_in_dim(routes, tp_rank * seq_count, seq_count, 0)
    own_weights = lax.dynamic_slice_in_dim(route_weights, tp_rank * seq_count, seq_count, 0)
    holder = jnp.arange(devices, dtype=jnp.int32) // tp_size
    picks = own_routes[None, :, :] == holder[:, None, None]
    scale = jnp.sum(jnp.where(picks, own_weights[None], 0.0), axis=-1)
    routed = jnp.sum(scale[:, :, None] * returned.astype(jnp.float32), axis=0)
    hidden_out = (own_resid.astype(jnp.float32) + rms_scale(routed, norm_gains[3])).astype(
        jnp.bfloat16
    )
    return (hidden_out, new_latent, new_rope)


LANES = 128
BIG = 20 * 10**9


def dma_chunks(ref, buffer, count):
    rows = ref.shape[0] // count
    return [(ref.at[pl.ds(i * rows, rows)], buffer.at[pl.ds(i * rows, rows)]) for i in range(count)]


def lane_chunk(value, index):
    return value[:, index * LANES : (index + 1) * LANES]


def mean_scale(value, count):
    return lax.rsqrt(jnp.sum(value * value, keepdims=True) / count + EPSILON)


def query_kernel(
    tokens,
    gains,
    lengths,
    w_rope,
    w_query,
    w_query_rope,
    w_latent,
    w_key,
    rows,
    own_tokens,
    gain_rows,
    new_rope,
    table,
    rope_buf,
    length_buf,
    tokens_buf,
    gains_buf,
    query_buf,
    query_rope_buf,
    latent_buf,
    key_buf,
    token_rows,
    sems,
):
    group_rows, width = tokens.shape
    heads, nope, latent = w_key.shape
    pieces = width // LANES
    per_head = latent // LANES
    block = rows.shape[0] // group_rows
    query_steps = dma_chunks(w_query, query_buf, 4)
    key_steps = dma_chunks(w_key, key_buf, heads)
    rot_steps = dma_chunks(w_query_rope, query_rope_buf, 2)
    latent_steps = dma_chunks(w_latent, latent_buf, 1)
    rope_steps = [(w_rope, rope_buf)]
    first_steps = [(tokens, tokens_buf), (gains, gains_buf), (lengths, length_buf)]
    copies = [
        pltpu.make_async_copy(src, dst, sems.at[i])
        for i, (src, dst) in enumerate(
            first_steps + query_steps + key_steps + rot_steps + latent_steps + rope_steps
        )
    ]
    for copy in copies:
        copy.start()
    pending = iter(copies)
    rank = lax.axis_index("tp")

    next(pending).wait()
    next(pending).wait()
    tokens_f = tokens_buf[...].astype(jnp.float32)
    gains = gains_buf
    power = jnp.sum(tokens_f * tokens_f, axis=-1, keepdims=True) / width
    normed = (tokens_f * lax.rsqrt(power + EPSILON) * gains[0:1, :]).astype(jnp.bfloat16)
    for k in range(pieces):
        token_rows[pl.ds(k, group_rows, stride=pieces), :] = lane_chunk(tokens_f, k)
        gain_rows[pl.ds(k, gains.shape[0], stride=pieces), :] = lane_chunk(gains[...], k)
    own_tokens[...] = token_rows[pl.ds(pl.multiple_of(rank * pieces, pieces), pieces), :]
    next(pending).wait()
    half = LANES // 2
    lane = lax.broadcasted_iota(jnp.int32, (1, LANES), 1)
    exponent = (lane % (half // 2)).astype(jnp.float32) * (-math.log(ROTARY_BASE) / (half // 2))
    angles = length_buf[0].astype(jnp.float32) * jnp.exp(exponent)
    sine = jnp.sin(angles)
    table[0:1, :] = jnp.cos(angles)
    table[1:2, :] = jnp.where(lane % half < half // 2, -sine, sine)

    def project(buffer, steps):
        depth = width // len(steps)
        total = None
        for i in range(len(steps)):
            next(pending).wait()
            part = jnp.dot(
                normed[:, i * depth : (i + 1) * depth],
                buffer[pl.ds(i * depth, depth), :],
                preferred_element_type=jnp.float32,
            )
            total = part if total is None else total + part
        return total

    q_nope = project(query_buf, query_steps).astype(jnp.bfloat16)
    for h in range(heads):
        next(pending).wait()
        q_latent = jnp.dot(
            q_nope[:, h * nope : (h + 1) * nope], key_buf[h], preferred_element_type=jnp.float32
        )
        for k in range(per_head):
            rows[pl.ds(h * per_head + k, group_rows, stride=block), :] = lane_chunk(q_latent, k)
    q_rot = project(query_rope_buf, rot_steps)
    low = lax.broadcasted_iota(jnp.int32, (group_rows, LANES), 1) < half
    base = heads * per_head
    for h in range(heads):
        pair = lane_chunk(q_rot, h // 2)
        turned = pltpu.roll(pair, half, 1)
        twice = jnp.where(low, pair, turned) if h % 2 == 0 else jnp.where(low, turned, pair)
        rows[pl.ds(base + h, group_rows, stride=block), :] = twice
    latent_cols = project(latent_buf, latent_steps)
    for k in range(base + heads, block):
        rows[pl.ds(k, group_rows, stride=block), :] = latent_cols
    next(pending).wait()
    rope_raw = lax.dot_general(
        normed, rope_buf[...], (((1,), (1,)), ((), ())), preferred_element_type=jnp.float32
    )
    mine = lax.broadcasted_iota(jnp.int32, rope_raw.shape, 0) == rank
    rope_raw = jnp.sum(jnp.where(mine, rope_raw, 0.0), axis=0, keepdims=True)
    rope_raw = rope_raw.astype(jnp.bfloat16).astype(jnp.float32)
    twice = jnp.concatenate([rope_raw, rope_raw], axis=1)
    turned = twice * table[0:1, :] + pltpu.roll(twice, half // 2, 1) * table[1:2, :]
    new_rope[...] = turned[:, :half].astype(jnp.bfloat16)


def pack_kernel(rows, send):
    block = send.shape[1]
    for j in range(send.shape[0]):
        send[j] = rows[pl.ds(j * block, block), :].astype(jnp.bfloat16)


def attend_kernel(
    length,
    received,
    cache,
    cache_rope,
    table,
    gain,
    rope_new,
    send,
    new_latent,
    rows,
    extra,
    rot_rows,
    queries,
    score_scale,
):
    sources, block, _ = received.shape
    latent = cache.shape[1]
    per_head = latent // LANES
    rope = cache_rope.shape[0]
    heads = queries.shape[0]
    here = heads // sources
    base = here * per_head
    tail = block - base
    for j in range(sources):
        piece = received[j].astype(jnp.float32)
        rows[pl.ds(j * base, base), :] = piece[:base]
        extra[pl.ds(j * tail, tail), :] = piece[base:]
    for k in range(per_head):
        queries[:, k * LANES : (k + 1) * LANES] = rows[
            pl.ds(k, heads, stride=per_head), :
        ].astype(jnp.bfloat16)
    for j in range(sources):
        rot_rows[pl.ds(j * here, here), :] = extra[pl.ds(j * tail, here), :]
    latent_raw = extra[pl.ds(here, sources, stride=tail), :]
    latent_f = (latent_raw * mean_scale(latent_raw, latent) * gain[...]).astype(jnp.bfloat16)
    latent_f = latent_f.astype(jnp.float32)
    for k in range(per_head):
        new_latent[:, k * LANES : (k + 1) * LANES] = latent_f[k : k + 1, :].astype(jnp.bfloat16)
    rot = rot_rows[...]
    q_pe = rot * table[0:1, :] + pltpu.roll(rot, LANES // 4, 1) * table[1:2, :]
    q_pe = q_pe[:, :rope].astype(jnp.bfloat16)
    q = queries[...]
    scores = lax.dot_general(
        q, cache[...], (((1,), (1,)), ((), ())), preferred_element_type=jnp.float32
    )
    scores = scores + jnp.dot(q_pe, cache_rope[...], preferred_element_type=jnp.float32)
    scores = scores * score_scale
    q_f = q.astype(jnp.float32)
    products = lane_chunk(q_f, 0) * latent_f[0:1, :]
    for k in range(1, per_head):
        products = products + lane_chunk(q_f, k) * latent_f[k : k + 1, :]
    own = jnp.sum(products, axis=1, keepdims=True)
    own = own + jnp.sum(
        q_pe.astype(jnp.float32) * rope_new[...].astype(jnp.float32), axis=1, keepdims=True
    )
    own = own * score_scale
    visible = lax.broadcasted_iota(jnp.int32, scores.shape, 1) < length[0]
    top = jnp.maximum(jnp.max(jnp.where(visible, scores, -jnp.inf), axis=1, keepdims=True), own)
    weights = jnp.where(visible, jnp.exp(scores - top), 0.0)
    own_weight = jnp.exp(own - top)
    total = jnp.sum(weights, axis=1, keepdims=True) + own_weight
    probs = (weights / total).astype(jnp.bfloat16)
    own_prob = (own_weight / total).astype(jnp.bfloat16).astype(jnp.float32)
    attended = jnp.dot(probs, cache[...], preferred_element_type=jnp.float32)
    for k in range(per_head):
        rows[pl.ds(k, heads, stride=per_head), :] = (
            lane_chunk(attended, k) + own_prob * latent_f[k : k + 1, :]
        )
    for j in range(sources):
        send[j] = rows[pl.ds(j * base, base), :].astype(jnp.bfloat16)


def output_kernel(received, w_value, w_output, send, rows, term_rows):
    sources, block, _ = received.shape
    heads, latent, _ = w_value.shape
    per_head = latent // LANES
    pieces = w_output.shape[1] // LANES
    for j in range(sources):
        rows[pl.ds(j * block, block), :] = received[j].astype(jnp.float32)
    values = []
    for h in range(heads):
        attended = jnp.concatenate(
            [
                rows[pl.ds(h * per_head + k, sources, stride=block), :].astype(jnp.bfloat16)
                for k in range(per_head)
            ],
            axis=1,
        )
        values.append(
            jnp.dot(attended, w_value[h], preferred_element_type=jnp.float32).astype(jnp.bfloat16)
        )
    values = jnp.concatenate(values, axis=1)
    step = 4
    for c in range(0, pieces, step):
        term = jnp.dot(
            values,
            w_output[:, c * LANES : (c + step) * LANES],
            preferred_element_type=jnp.float32,
        )
        for k in range(step):
            term_rows[pl.ds(c + k, sources, stride=pieces), :] = lane_chunk(term, k)
    for j in range(sources):
        send[j] = term_rows[pl.ds(j * pieces, pieces), :].astype(jnp.bfloat16)


def resid_kernel(routes, route_weights, received, own_tokens, gain_rows, send, resid, scales):
    mine = lax.broadcasted_iota(jnp.int32, routes.shape, 1) == lax.axis_index("tp")
    named = jnp.sum(jnp.where(mine, routes[...], 0), axis=1, keepdims=True)
    weight = jnp.sum(jnp.where(mine, route_weights[...], 0.0), axis=1, keepdims=True)
    for e in range(scales.shape[0]):
        total = jnp.sum(jnp.where(named == e, weight, 0.0), axis=0, keepdims=True)
        scales[e : e + 1, :] = jnp.broadcast_to(total, (1, LANES))
    pieces = received.shape[1]
    count = pieces * LANES
    mixed = received[0].astype(jnp.float32)
    for j in range(1, received.shape[0]):
        mixed = mixed + received[j].astype(jnp.float32)
    after = own_tokens[...] + mixed * mean_scale(mixed, count) * gain_rows[pieces : 2 * pieces]
    after = after.astype(jnp.bfloat16).astype(jnp.float32)
    resid[...] = after
    expert_in = after * mean_scale(after, count) * gain_rows[2 * pieces : 3 * pieces]
    expert_in = expert_in.astype(jnp.bfloat16)
    for j in range(send.shape[0]):
        send[j] = expert_in


def expert_kernel(received, w_gate, w_up, w_down, send, rows, inputs):
    sources, pieces, _ = received.shape
    for j in range(sources):
        rows[pl.ds(j * pieces, pieces), :] = received[j].astype(jnp.float32)
    for k in range(pieces):
        inputs[:, k * LANES : (k + 1) * LANES] = rows[
            pl.ds(k, sources, stride=pieces), :
        ].astype(jnp.bfloat16)
    gate = jnp.dot(inputs[...], w_gate[...], preferred_element_type=jnp.float32)
    up = jnp.dot(inputs[...], w_up[...], preferred_element_type=jnp.float32)
    inner = (gate / (1.0 + jnp.exp(-gate)) * up).astype(jnp.bfloat16)
    step = 4
    for c in range(0, pieces, step):
        piece = jnp.dot(
            inner, w_down[:, c * LANES : (c + step) * LANES], preferred_element_type=jnp.float32
        )
        for k in range(step):
            rows[pl.ds(c + k, sources, stride=pieces), :] = lane_chunk(piece, k)
    for j in range(sources):
        send[j] = rows[pl.ds(j * pieces, pieces), :].astype(jnp.bfloat16)


def final_kernel(scales, received, resid, gain_rows, hidden):
    sources, pieces, _ = received.shape
    experts = scales.shape[0]
    per_expert = sources // experts
    routed = None
    for e in range(experts):
        block = received[e * per_expert].astype(jnp.float32)
        for b in range(1, per_expert):
            block = block + received[e * per_expert + b].astype(jnp.float32)
        part = block * scales[e : e + 1, :]
        routed = part if routed is None else routed + part
    out = resid[...] + routed * mean_scale(routed, pieces * LANES) * gain_rows[3 * pieces :]
    for k in range(pieces):
        hidden[:, k * LANES : (k + 1) * LANES] = out[k : k + 1, :].astype(jnp.bfloat16)


def kernel_call(body, outs, specs, scratch, megabytes, flops, name):
    bytes_moved = 32 * 1024 * 1024 if flops >= BIG else 4 * 1024 * 1024
    return pl.pallas_call(
        body,
        out_shape=outs,
        in_specs=specs,
        out_specs=jax.tree.map(lambda _: pl.BlockSpec(memory_space=pltpu.VMEM), outs),
        scratch_shapes=scratch,
        compiler_params=pltpu.CompilerParams(vmem_limit_bytes=megabytes * 1024 * 1024),
        cost_estimate=pl.CostEstimate(
            flops=flops, bytes_accessed=bytes_moved, transcendentals=0
        ),
        name=name,
    )


def lanes_fit(w_key_up, w_value_up, w_latent_down, w_rope_down, cache_latent, tp_size):
    return (
        cache_latent.shape[0] == 1
        and w_latent_down.shape[1] == LANES
        and w_key_up.shape[0] % 2 == 0
        and w_key_up.shape[1] == LANES
        and w_value_up.shape[2] == LANES
        and 2 * w_rope_down.shape[1] == LANES
        and w_key_up.shape[2] == tp_size * LANES
        and w_key_up.shape[0] * w_key_up.shape[2] // LANES % 8 == 0
        and w_key_up.shape[0] < 8
    )


def on_device_fused(
    tokens,
    norm_gains,
    w_query,
    w_query_rope,
    w_key_up,
    w_value_up,
    w_output,
    w_latent_down,
    latent_gain,
    w_rope_down,
    cache_latent,
    cache_rope,
    lengths,
    routes,
    route_weights,
    w_gate,
    w_up,
    w_down,
):
    tp_size = lax.axis_size("tp")
    ep_size = lax.axis_size("ep")
    devices = tp_size * ep_size
    heads_here, nope, latent = w_key_up.shape
    heads = heads_here * tp_size
    group_rows, width = tokens.shape
    rope = w_rope_down.shape[1]
    cached = cache_latent.shape[1]
    pieces = width // LANES
    per_head = latent // LANES
    base = heads_here * per_head
    block = base + 8
    bf16, f32 = jnp.bfloat16, jnp.float32
    vmem = pl.BlockSpec(memory_space=pltpu.VMEM)
    smem = pl.BlockSpec(memory_space=pltpu.SMEM)
    hbm = pl.BlockSpec(memory_space=pltpu.HBM)
    shape = jax.ShapeDtypeStruct

    rows, own_tokens, gain_rows, new_rope, table = kernel_call(
        query_kernel,
        (
            shape((group_rows * block, LANES), f32),
            shape((pieces, LANES), f32),
            shape((norm_gains.shape[0] * pieces, LANES), f32),
            shape((1, rope), bf16),
            shape((2, LANES), f32),
        ),
        [hbm] * 8,
        [
            pltpu.VMEM((rope, width), bf16),
            pltpu.SMEM(lengths.shape, jnp.int32),
            pltpu.VMEM(tokens.shape, bf16),
            pltpu.VMEM(norm_gains.shape, f32),
            pltpu.VMEM(w_query.shape, bf16),
            pltpu.VMEM(w_query_rope.shape, bf16),
            pltpu.VMEM(w_latent_down.shape, bf16),
            pltpu.VMEM(w_key_up.shape, bf16),
            pltpu.VMEM((group_rows * pieces, LANES), f32),
            pltpu.SemaphoreType.DMA((11 + heads_here,)),
        ],
        61,
        2 * group_rows * w_query.size,
        "queries",
    )(
        tokens,
        norm_gains,
        lengths,
        w_rope_down.T,
        w_query,
        w_query_rope,
        w_latent_down,
        w_key_up,
    )
    send = kernel_call(
        pack_kernel,
        shape((tp_size, block, LANES), bf16),
        [vmem],
        [],
        2,
        BIG,
        "pack",
    )(rows)
    received = lax.all_to_all(send, "tp", split_axis=0, concat_axis=0, tiled=True)
    send, new_latent = kernel_call(
        functools.partial(attend_kernel, score_scale=(nope + rope) ** (-0.5)),
        (shape((tp_size, base, LANES), bf16), shape((1, latent), bf16)),
        [smem] + [vmem] * 6,
        [
            pltpu.VMEM((tp_size * base, LANES), f32),
            pltpu.VMEM((tp_size * 8, LANES), f32),
            pltpu.VMEM((heads, LANES), f32),
            pltpu.VMEM((heads, latent), bf16),
        ],
        8,
        4 * heads * cached * latent,
        "attend",
    )(
        lengths,
        received,
        cache_latent[0],
        cache_rope[0].T,
        table,
        latent_gain.reshape(-1, LANES),
        new_rope,
    )
    received = lax.all_to_all(send, "tp", split_axis=0, concat_axis=0, tiled=True)
    send = kernel_call(
        output_kernel,
        shape((tp_size, pieces, LANES), bf16),
        [vmem] * 3,
        [
            pltpu.VMEM((tp_size * base, LANES), f32),
            pltpu.VMEM((tp_size * pieces, LANES), f32),
        ],
        10,
        2 * group_rows * (w_output.size + w_value_up.size),
        "outputs",
    )(received, w_value_up, w_output)
    received = lax.all_to_all(send, "tp", split_axis=0, concat_axis=0, tiled=True)
    send, resid, scales = kernel_call(
        resid_kernel,
        (
            shape((devices, pieces, LANES), bf16),
            shape((pieces, LANES), f32),
            shape((ep_size, LANES), f32),
        ),
        [vmem] * 5,
        [],
        4,
        10 * tp_size * width,
        "resid",
    )(routes.T, route_weights.T, received, own_tokens, gain_rows)
    everyone = ("ep", "tp")
    received = lax.all_to_all(send, everyone, split_axis=0, concat_axis=0, tiled=True)
    send = kernel_call(
        expert_kernel,
        shape((devices, pieces, LANES), bf16),
        [vmem] * 4,
        [
            pltpu.VMEM((devices * pieces, LANES), f32),
            pltpu.VMEM((devices, width), bf16),
        ],
        12,
        6 * devices * w_gate.size,
        "experts",
    )(received, w_gate[0], w_up[0], w_down[0])
    received = lax.all_to_all(send, everyone, split_axis=0, concat_axis=0, tiled=True)
    hidden = kernel_call(
        final_kernel,
        shape((1, width), bf16),
        [vmem] * 4,
        [],
        4,
        2 * devices * width,
        "final",
    )(scales, received, resid, gain_rows)
    return hidden, new_latent, new_rope


def on_device(*arrays):
    w_key_up, w_value_up, w_latent_down, w_rope_down = (arrays[i] for i in (4, 5, 7, 9))
    if lanes_fit(
        w_key_up, w_value_up, w_latent_down, w_rope_down, arrays[10], lax.axis_size("tp")
    ):
        return on_device_fused(*arrays)
    return on_device_plain(*arrays)


def solution(mesh):
    in_specs = (
        P("ep", None),
        P(),
        P(None, "tp"),
        P(None, "tp"),
        P("tp", None, None),
        P("tp", None, None),
        P("tp", None),
        P(None, "tp"),
        P(),
        P(),
        P(("ep", "tp"), None, None),
        P(("ep", "tp"), None, None),
        P(("ep", "tp")),
        P("ep", None),
        P("ep", None),
        P("ep", None, "tp"),
        P("ep", None, "tp"),
        P("ep", "tp", None),
    )
    out_specs = (P(("ep", "tp"), None), P(("ep", "tp"), None), P(("ep", "tp"), None))
    return jax.shard_map(
        on_device, mesh=mesh, in_specs=in_specs, out_specs=out_specs, check_vma=False
    )
```

```python
import functools
import math

import jax
import jax.numpy as jnp
from jax import lax
from jax.experimental import pallas as pl
from jax.experimental.pallas import tpu as pltpu
from jax.sharding import PartitionSpec as P

EPSILON = 1e-06
ROTARY_BASE = 500000.0


def rms_scale(source, gain_row):
    values_f = source.astype(jnp.float32)
    return (
        values_f
        * lax.rsqrt(jnp.mean(values_f * values_f, axis=-1, keepdims=True) + EPSILON)
        * gain_row
    )


def rotate(source, position):
    half_width = source.shape[-1] // 2
    frequency = ROTARY_BASE ** (-jnp.arange(half_width, dtype=jnp.float32) / half_width)
    angles = position[..., None] * frequency
    first_half = source[..., :half_width]
    second_half = source[..., half_width:]
    return jnp.concatenate(
        [
            first_half * jnp.cos(angles) - second_half * jnp.sin(angles),
            second_half * jnp.cos(angles) + first_half * jnp.sin(angles),
        ],
        axis=-1,
    )


def attend(q_latent, q_pe, cache_lat, cache_rp, lat_new, rope_new, lengths, score_scale):
    scores = (
        jnp.einsum("shc,spc->shp", q_latent, cache_lat, preferred_element_type=jnp.float32)
        + jnp.einsum("shr,spr->shp", q_pe, cache_rp, preferred_element_type=jnp.float32)
    ) * score_scale
    own_score = (
        jnp.einsum("shc,sc->sh", q_latent, lat_new, preferred_element_type=jnp.float32)
        + jnp.einsum("shr,sr->sh", q_pe, rope_new, preferred_element_type=jnp.float32)
    ) * score_scale
    visible = (
        jnp.arange(cache_lat.shape[1], dtype=jnp.int32)[None, None, :] < lengths[:, None, None]
    )
    row_max = jnp.maximum(jnp.max(jnp.where(visible, scores, -jnp.inf), axis=-1), own_score)
    weights = jnp.where(visible, jnp.exp(scores - row_max[..., None]), 0.0)
    own_weight = jnp.exp(own_score - row_max)
    denominator = jnp.sum(weights, axis=-1) + own_weight
    probabilities = (weights / denominator[..., None]).astype(jnp.bfloat16)
    own_prob = (own_weight / denominator).astype(jnp.bfloat16)
    attended = jnp.einsum(
        "shp,spc->shc", probabilities, cache_lat, preferred_element_type=jnp.float32
    )
    attended = (
        attended + own_prob.astype(jnp.float32)[..., None] * lat_new.astype(jnp.float32)[:, None, :]
    )
    return attended.astype(jnp.bfloat16)


def to_sequences(rows, tp_size, seq_count):
    blocks = rows.reshape(tp_size, seq_count, rows.shape[1])
    return lax.all_to_all(blocks, "tp", split_axis=0, concat_axis=0, tiled=True)


def on_device_plain(
    tokens,
    norm_gains,
    w_query,
    w_query_rope,
    w_key_up,
    w_value_up,
    w_output,
    w_latent_down,
    latent_gain,
    w_rope_down,
    cache_latent,
    cache_rope,
    lengths,
    routes,
    route_weights,
    w_gate,
    w_up,
    w_down,
):
    group_rows = tokens.shape[0]
    seq_count = cache_latent.shape[0]
    heads_here = w_key_up.shape[0]
    nope_width = w_key_up.shape[1]
    rope_width = w_rope_down.shape[1]
    tp_size = lax.axis_size("tp")
    tp_rank = lax.axis_index("tp")
    normed = rms_scale(tokens, norm_gains[0]).astype(jnp.bfloat16)
    q_nope = jnp.dot(normed, w_query, preferred_element_type=jnp.float32).astype(jnp.bfloat16)
    q_nope = q_nope.reshape(group_rows, heads_here, nope_width)
    q_latent = jnp.einsum("thn,hnc->thc", q_nope, w_key_up, preferred_element_type=jnp.float32)
    q_latent = q_latent.astype(jnp.bfloat16).reshape(group_rows, -1)
    q_rot = jnp.dot(normed, w_query_rope, preferred_element_type=jnp.float32).astype(jnp.bfloat16)
    latent_cols = jnp.dot(normed, w_latent_down, preferred_element_type=jnp.float32).astype(
        jnp.bfloat16
    )
    q_cols, rot_cols = q_latent.shape[1], q_rot.shape[1]
    packed = jnp.concatenate([q_latent, q_rot, latent_cols], axis=1)
    packed = to_sequences(packed, tp_size, seq_count)
    q_mine = packed[:, :, :q_cols].transpose(1, 0, 2).reshape(seq_count, -1)
    rot_mine = packed[:, :, q_cols : q_cols + rot_cols].transpose(1, 0, 2).reshape(seq_count, -1)
    latent_raw = packed[:, :, q_cols + rot_cols :].transpose(1, 0, 2).reshape(seq_count, -1)
    heads_all = rot_mine.shape[1] // rope_width
    own_normed = lax.dynamic_slice_in_dim(normed, tp_rank * seq_count, seq_count, 0)
    rope_raw = jnp.dot(own_normed, w_rope_down, preferred_element_type=jnp.float32).astype(
        jnp.bfloat16
    )
    new_latent = rms_scale(latent_raw, latent_gain).astype(jnp.bfloat16)
    position = lengths.astype(jnp.float32)
    new_rope = rotate(rope_raw.astype(jnp.float32), position).astype(jnp.bfloat16)
    q_pe = rotate(
        rot_mine.reshape(seq_count, heads_all, rope_width).astype(jnp.float32), position[:, None]
    )
    q_pe = q_pe.astype(jnp.bfloat16)
    score_scale = (nope_width + rope_width) ** (-0.5)
    attended = attend(
        q_mine.reshape(seq_count, heads_all, -1),
        q_pe,
        cache_latent,
        cache_rope,
        new_latent,
        new_rope,
        lengths,
        score_scale,
    )
    head_latent = lax.all_to_all(
        attended.reshape(seq_count, -1), "tp", split_axis=1, concat_axis=0, tiled=True
    )
    values = (
        jnp.einsum(
            "thc,hcv->thv",
            head_latent.reshape(group_rows, heads_here, -1),
            w_value_up,
            preferred_element_type=jnp.float32,
        )
        .astype(jnp.bfloat16)
        .reshape(group_rows, -1)
    )
    head_term = jnp.dot(values, w_output, preferred_element_type=jnp.float32)
    terms = to_sequences(head_term.astype(jnp.bfloat16), tp_size, seq_count)
    mixed = jnp.sum(terms.astype(jnp.float32), axis=0)
    own_tokens = lax.dynamic_slice_in_dim(tokens, tp_rank * seq_count, seq_count, 0)
    own_resid = (own_tokens.astype(jnp.float32) + rms_scale(mixed, norm_gains[1])).astype(
        jnp.bfloat16
    )
    expert_in = rms_scale(own_resid, norm_gains[2]).astype(jnp.bfloat16)
    everyone = ("ep", "tp")
    devices = lax.axis_size("ep") * tp_size
    copies = jnp.broadcast_to(expert_in[None], (devices,) + expert_in.shape)
    arrived = lax.all_to_all(copies, everyone, split_axis=0, concat_axis=0, tiled=True)
    arrived = arrived.reshape(devices * seq_count, -1)
    gate_sum = jnp.dot(arrived, w_gate[0], preferred_element_type=jnp.float32)
    up_sum = jnp.dot(arrived, w_up[0], preferred_element_type=jnp.float32)
    hidden_units = (jax.nn.silu(gate_sum) * up_sum).astype(jnp.bfloat16)
    pieces = jnp.dot(hidden_units, w_down[0], preferred_element_type=jnp.float32).astype(
        jnp.bfloat16
    )
    pieces = pieces.reshape(devices, seq_count, -1)
    returned = lax.all_to_all(pieces, everyone, split_axis=0, concat_axis=0, tiled=True)
    own_routes = lax.dynamic_slice_in_dim(routes, tp_rank * seq_count, seq_count, 0)
    own_weights = lax.dynamic_slice_in_dim(route_weights, tp_rank * seq_count, seq_count, 0)
    holder = jnp.arange(devices, dtype=jnp.int32) // tp_size
    picks = own_routes[None, :, :] == holder[:, None, None]
    scale = jnp.sum(jnp.where(picks, own_weights[None], 0.0), axis=-1)
    routed = jnp.sum(scale[:, :, None] * returned.astype(jnp.float32), axis=0)
    hidden_out = (own_resid.astype(jnp.float32) + rms_scale(routed, norm_gains[3])).astype(
        jnp.bfloat16
    )
    return (hidden_out, new_latent, new_rope)


LANES = 128
BIG = 20 * 10**9


def lane_chunk(value, index):
    return value[:, index * LANES : (index + 1) * LANES]


def mean_scale(value, count):
    return lax.rsqrt(jnp.sum(value * value, keepdims=True) / count + EPSILON)


def angle_kernel(lengths, table):
    half = LANES // 2
    lane = lax.broadcasted_iota(jnp.int32, (1, LANES), 1)
    exponent = (lane % (half // 2)).astype(jnp.float32) * (-math.log(ROTARY_BASE) / (half // 2))
    angles = lengths[0].astype(jnp.float32) * jnp.exp(exponent)
    sine = jnp.sin(angles)
    table[0:1, :] = jnp.cos(angles)
    table[1:2, :] = jnp.where(lane % half < half // 2, -sine, sine)


def query_kernel(
    table,
    tokens,
    gains,
    w_query,
    w_key,
    w_query_rope,
    w_latent,
    w_rope,
    send,
    rope_row,
    token_rows,
    gain_rows,
    rows,
):
    group_rows, width = tokens.shape
    heads, nope, latent = w_key.shape
    pieces = width // LANES
    per_head = latent // LANES
    block = send.shape[1]
    base = heads * per_head
    tokens_f = tokens[...].astype(jnp.float32)
    power = jnp.sum(tokens_f * tokens_f, axis=-1, keepdims=True) / width
    normed = (tokens_f * lax.rsqrt(power + EPSILON) * gains[0:1, :]).astype(jnp.bfloat16)
    q_nope = jnp.dot(normed, w_query[...], preferred_element_type=jnp.float32)
    q_nope = q_nope.astype(jnp.bfloat16)
    q_rot = jnp.dot(normed, w_query_rope[...], preferred_element_type=jnp.float32)
    latent_cols = jnp.dot(normed, w_latent[...], preferred_element_type=jnp.float32)
    rope_raw = lax.dot_general(
        normed, w_rope[...], (((1,), (1,)), ((), ())), preferred_element_type=jnp.float32
    )
    for h in range(heads):
        q_latent = jnp.dot(
            q_nope[:, h * nope : (h + 1) * nope], w_key[h], preferred_element_type=jnp.float32
        )
        for k in range(per_head):
            rows[pl.ds(h * per_head + k, group_rows, stride=block), :] = lane_chunk(q_latent, k)
    half = LANES // 2
    low = lax.broadcasted_iota(jnp.int32, (group_rows, LANES), 1) < half
    for h in range(heads):
        pair = lane_chunk(q_rot, h // 2)
        turned = pltpu.roll(pair, half, 1)
        twice = jnp.where(low, pair, turned) if h % 2 == 0 else jnp.where(low, turned, pair)
        rows[pl.ds(base + h, group_rows, stride=block), :] = twice
    for k in range(base + heads, block):
        rows[pl.ds(k, group_rows, stride=block), :] = latent_cols
    for k in range(pieces):
        token_rows[pl.ds(k, group_rows, stride=pieces), :] = lane_chunk(tokens_f, k)
        gain_rows[pl.ds(k, gains.shape[0], stride=pieces), :] = lane_chunk(gains[...], k)
    mine = lax.broadcasted_iota(jnp.int32, rope_raw.shape, 0) == lax.axis_index("tp")
    rope_raw = jnp.sum(jnp.where(mine, rope_raw, 0.0), axis=0, keepdims=True)
    rope_raw = rope_raw.astype(jnp.bfloat16).astype(jnp.float32)
    twice = jnp.concatenate([rope_raw, rope_raw], axis=1)
    turned = twice * table[0:1, :] + pltpu.roll(twice, half // 2, 1) * table[1:2, :]
    rope_row[...] = turned.astype(jnp.bfloat16).astype(jnp.float32)
    for j in range(group_rows):
        send[j] = rows[pl.ds(j * block, block), :].astype(jnp.bfloat16)


def attend_kernel(
    length,
    received,
    cache,
    cache_rope,
    table,
    gain,
    rope_row,
    send,
    latent_rows,
    rows,
    extra,
    rot_rows,
    queries,
    score_scale,
):
    sources, block, _ = received.shape
    latent = cache.shape[1]
    per_head = latent // LANES
    rope = cache_rope.shape[0]
    heads = queries.shape[0]
    here = heads // sources
    base = here * per_head
    tail = block - base
    for j in range(sources):
        piece = received[j].astype(jnp.float32)
        rows[pl.ds(j * base, base), :] = piece[:base]
        extra[pl.ds(j * tail, tail), :] = piece[base:]
    for k in range(per_head):
        queries[:, k * LANES : (k + 1) * LANES] = rows[
            pl.ds(k, heads, stride=per_head), :
        ].astype(jnp.bfloat16)
    for j in range(sources):
        rot_rows[pl.ds(j * here, here), :] = extra[pl.ds(j * tail, here), :]
    latent_raw = extra[pl.ds(here, sources, stride=tail), :]
    latent_f = (latent_raw * mean_scale(latent_raw, latent) * gain[...]).astype(jnp.bfloat16)
    latent_f = latent_f.astype(jnp.float32)
    latent_rows[...] = latent_f
    rot = rot_rows[...]
    q_pe = rot * table[0:1, :] + pltpu.roll(rot, LANES // 4, 1) * table[1:2, :]
    q_pe = q_pe[:, :rope].astype(jnp.bfloat16)
    q = queries[...]
    scores = lax.dot_general(
        q, cache[...], (((1,), (1,)), ((), ())), preferred_element_type=jnp.float32
    )
    scores = scores + jnp.dot(q_pe, cache_rope[...], preferred_element_type=jnp.float32)
    scores = scores * score_scale
    q_f = q.astype(jnp.float32)
    products = lane_chunk(q_f, 0) * latent_f[0:1, :]
    for k in range(1, per_head):
        products = products + lane_chunk(q_f, k) * latent_f[k : k + 1, :]
    own = jnp.sum(products, axis=1, keepdims=True)
    own = own + jnp.sum(
        q_pe.astype(jnp.float32) * rope_row[:, :rope], axis=1, keepdims=True
    )
    own = own * score_scale
    visible = lax.broadcasted_iota(jnp.int32, scores.shape, 1) < length[0]
    top = jnp.maximum(jnp.max(jnp.where(visible, scores, -jnp.inf), axis=1, keepdims=True), own)
    weights = jnp.where(visible, jnp.exp(scores - top), 0.0)
    own_weight = jnp.exp(own - top)
    total = jnp.sum(weights, axis=1, keepdims=True) + own_weight
    probs = (weights / total).astype(jnp.bfloat16)
    own_prob = (own_weight / total).astype(jnp.bfloat16).astype(jnp.float32)
    attended = jnp.dot(probs, cache[...], preferred_element_type=jnp.float32)
    for k in range(per_head):
        rows[pl.ds(k, heads, stride=per_head), :] = (
            lane_chunk(attended, k) + own_prob * latent_f[k : k + 1, :]
        )
    for j in range(sources):
        send[j] = rows[pl.ds(j * base, base), :].astype(jnp.bfloat16)


def output_kernel(received, w_value, w_output, send, rows, term_rows):
    sources, block, _ = received.shape
    heads, latent, _ = w_value.shape
    per_head = latent // LANES
    pieces = w_output.shape[1] // LANES
    for j in range(sources):
        rows[pl.ds(j * block, block), :] = received[j].astype(jnp.float32)
    values = []
    for h in range(heads):
        attended = jnp.concatenate(
            [
                rows[pl.ds(h * per_head + k, sources, stride=block), :].astype(jnp.bfloat16)
                for k in range(per_head)
            ],
            axis=1,
        )
        values.append(
            jnp.dot(attended, w_value[h], preferred_element_type=jnp.float32).astype(jnp.bfloat16)
        )
    values = jnp.concatenate(values, axis=1)
    step = 4
    for c in range(0, pieces, step):
        term = jnp.dot(
            values,
            w_output[:, c * LANES : (c + step) * LANES],
            preferred_element_type=jnp.float32,
        )
        for k in range(step):
            term_rows[pl.ds(c + k, sources, stride=pieces), :] = lane_chunk(term, k)
    for j in range(sources):
        send[j] = term_rows[pl.ds(j * pieces, pieces), :].astype(jnp.bfloat16)


def half_rows(core, count):
    return [core * count + i for i in range(count)]


def pair_kernel(keep, got, send):
    for i in range(send.shape[0]):
        total = keep[i].astype(jnp.float32) + got[i].astype(jnp.float32)
        send[i] = total.astype(jnp.bfloat16)


def pair_half_kernel(keep, got, send, half):
    pair_kernel(keep, got, send)
    for i, row in enumerate(half_rows(lax.axis_index("tp") % 2, half.shape[0])):
        half[i] = send[row]


def combine_kernel(*refs):
    full, half, total = refs[:-2], refs[-2], refs[-1]
    for i in range(total.shape[0]):
        value = jnp.zeros(total.shape[1:], jnp.float32)
        for ref in full:
            value = value + ref[i].astype(jnp.float32)
        total[i] = value.astype(jnp.bfloat16)
    for i, row in enumerate(half_rows(1 - lax.axis_index("tp") % 2, half.shape[0])):
        value = half[i].astype(jnp.float32)
        for ref in full:
            value = value + ref[row].astype(jnp.float32)
        total[row] = value.astype(jnp.bfloat16)


def join_kernel(*refs):
    joined = refs[-1]
    place = 0
    for ref in refs[:-1]:
        for i in range(ref.shape[0]):
            joined[place + i] = ref[i]
        place += ref.shape[0]


def row_scales(blocks, count):
    power = [jnp.sum(block * block, axis=0, keepdims=True) for block in blocks]
    power = jnp.sum(jnp.concatenate(power, axis=0), axis=1, keepdims=True) / count
    scale = lax.rsqrt(power + EPSILON)
    return [scale[i : i + 1, :] for i in range(len(blocks))]


def resid_kernel(
    routes,
    route_weights,
    token_rows,
    gain_rows,
    own,
    partial,
    got,
    send,
    half,
    resid,
    scales,
    after_rows,
):
    rank = lax.axis_index("tp")
    mine = lax.broadcasted_iota(jnp.int32, routes.shape, 1) == rank
    named = jnp.sum(jnp.where(mine, routes[...], 0), axis=1, keepdims=True)
    weight = jnp.sum(jnp.where(mine, route_weights[...], 0.0), axis=1, keepdims=True)
    for e in range(scales.shape[0]):
        total = jnp.sum(jnp.where(named == e, weight, 0.0), axis=0, keepdims=True)
        scales[e : e + 1, :] = jnp.broadcast_to(total, (1, LANES))
    count, pieces, _ = send.shape
    width = pieces * LANES
    mixed = [
        own[i].astype(jnp.float32)
        + (partial[i].astype(jnp.float32) + got[i].astype(jnp.float32))
        for i in range(count)
    ]
    gain = gain_rows[pieces : 2 * pieces, :]
    after = [
        (token_rows[i * pieces : (i + 1) * pieces, :] + mixed[i] * scale * gain)
        .astype(jnp.bfloat16)
        .astype(jnp.float32)
        for i, scale in enumerate(row_scales(mixed, width))
    ]
    gain = gain_rows[2 * pieces : 3 * pieces, :]
    for i, scale in enumerate(row_scales(after, width)):
        after_rows[i] = after[i]
        send[i] = (after[i] * scale * gain).astype(jnp.bfloat16)
    resid[...] = after_rows[rank]
    for i, row in enumerate(half_rows(rank % 2, half.shape[0])):
        half[i] = send[row]


def expert_kernel(own, mine, others, w_gate, w_up, w_down, keep, give, rows, inputs, masks):
    members, pieces, _ = own.shape
    rank = lax.axis_index("tp")
    core = rank % 2
    group = lax.axis_index("ep")
    pairs, last = masks
    blocks = [own[i] for i in range(members)]
    places = [group * members + i for i in range(members)]
    for source, side in ((mine, 1 - core), (others, core)):
        blocks += [source[i] for i in range(source.shape[0])]
        for low, high in pairs:
            other = group ^ jnp.where(side == 0, low, high)
            places += [other * members + i for i in range(members)]
        places += [(group ^ last) * members + row for row in half_rows(side, members // 2)]
    count = len(places)
    for i, block in enumerate(blocks):
        rows[pl.ds(i * pieces, pieces), :] = block.astype(jnp.float32)
    for k in range(pieces):
        inputs[:, k * LANES : (k + 1) * LANES] = rows[
            pl.ds(k, count, stride=pieces), :
        ].astype(jnp.bfloat16)
    gate = jnp.dot(inputs[...], w_gate[...], preferred_element_type=jnp.float32)
    up = jnp.dot(inputs[...], w_up[...], preferred_element_type=jnp.float32)
    inner = (gate / (1.0 + jnp.exp(-gate)) * up).astype(jnp.bfloat16)
    step = 4
    for k in range(0, pieces, step):
        piece = jnp.dot(
            inner, w_down[:, k * LANES : (k + step) * LANES], preferred_element_type=jnp.float32
        )
        piece = piece.astype(jnp.bfloat16).astype(jnp.float32)
        for j in range(step):
            rows[pl.ds(k + j, count, stride=pieces), :] = lane_chunk(piece, j)
    half = pieces // 2
    for i, place in enumerate(places):
        start = pl.multiple_of(i * pieces + core * half, half)
        keep[place] = rows[pl.ds(start, half), :]
        start = pl.multiple_of(i * pieces + (1 - core) * half, half)
        give[place] = rows[pl.ds(start, half), :].astype(jnp.bfloat16)


def final_kernel(
    scales, received, resid, gain_rows, latent_rows, rope_row, hidden, new_latent, new_rope
):
    for k in range(latent_rows.shape[0]):
        new_latent[:, k * LANES : (k + 1) * LANES] = latent_rows[k : k + 1, :].astype(
            jnp.bfloat16
        )
    new_rope[...] = rope_row[:, : new_rope.shape[1]].astype(jnp.bfloat16)
    sources, half, _ = received.shape
    pieces = 2 * half
    experts = scales.shape[0]
    per_expert = sources // experts
    parts = []
    for c in range(2):
        total = None
        for e in range(experts):
            block = received[e * per_expert + c].astype(jnp.float32)
            for b in range(c + 2, per_expert, 2):
                block = block + received[e * per_expert + b].astype(jnp.float32)
            part = block * scales[e : e + 1, :]
            total = part if total is None else total + part
        parts.append(total)
    routed = jnp.concatenate(parts, axis=0)
    out = resid[...] + routed * mean_scale(routed, pieces * LANES) * gain_rows[3 * pieces :]
    for k in range(pieces):
        hidden[:, k * LANES : (k + 1) * LANES] = out[k : k + 1, :].astype(jnp.bfloat16)


def kernel_call(body, outs, specs, scratch, megabytes, flops, name):
    bytes_moved = flops // BIG * 32 * 1024 * 1024 if flops >= BIG else min(flops, 4 * 1024 * 1024)
    return pl.pallas_call(
        body,
        out_shape=outs,
        in_specs=specs,
        out_specs=jax.tree.map(lambda _: pl.BlockSpec(memory_space=pltpu.VMEM), outs),
        scratch_shapes=scratch,
        compiler_params=pltpu.CompilerParams(vmem_limit_bytes=megabytes * 1024 * 1024),
        cost_estimate=pl.CostEstimate(
            flops=flops, bytes_accessed=bytes_moved, transcendentals=0
        ),
        name=name,
    )


def mask_pairs(size):
    return [(m, m - 1) for m in range(size - 1, 1, -2)], 1


def power_of_two(size):
    return size & (size - 1) == 0


def lanes_fit(w_key_up, w_value_up, w_latent_down, w_rope_down, cache_latent, tp_size):
    return (
        cache_latent.shape[0] == 1
        and power_of_two(tp_size)
        and power_of_two(lax.axis_size("ep"))
        and tp_size > 2
        and lax.axis_size("ep") > 1
        and w_latent_down.shape[1] == LANES
        and w_key_up.shape[0] % 2 == 0
        and w_key_up.shape[1] == LANES
        and w_value_up.shape[2] == LANES
        and 2 * w_rope_down.shape[1] == LANES
        and w_key_up.shape[2] == tp_size * LANES
        and w_key_up.shape[0] * w_key_up.shape[2] // LANES % 8 == 0
        and w_key_up.shape[0] < 8
    )


def on_device_fused(
    tokens,
    norm_gains,
    w_query,
    w_query_rope,
    w_key_up,
    w_value_up,
    w_output,
    w_latent_down,
    latent_gain,
    w_rope_down,
    cache_latent,
    cache_rope,
    lengths,
    routes,
    route_weights,
    w_gate,
    w_up,
    w_down,
):
    tp_size = lax.axis_size("tp")
    ep_size = lax.axis_size("ep")
    devices = tp_size * ep_size
    heads_here, nope, latent = w_key_up.shape
    heads = heads_here * tp_size
    chips = tp_size // 2
    group_rows, width = tokens.shape
    rope = w_rope_down.shape[1]
    cached = cache_latent.shape[1]
    pieces = width // LANES
    per_head = latent // LANES
    base = heads_here * per_head
    block = base + 8
    bf16, f32 = jnp.bfloat16, jnp.float32
    vmem = pl.BlockSpec(memory_space=pltpu.VMEM)
    smem = pl.BlockSpec(memory_space=pltpu.SMEM)
    shape = jax.ShapeDtypeStruct

    table = kernel_call(
        angle_kernel, shape((2, LANES), f32), [smem], [], 1, 2 * BIG, "angles"
    )(lengths)
    send, rope_row, token_rows, gain_rows = kernel_call(
        query_kernel,
        (
            shape((tp_size, block, LANES), bf16),
            shape((1, LANES), f32),
            shape((group_rows * pieces, LANES), f32),
            shape((norm_gains.shape[0] * pieces, LANES), f32),
        ),
        [vmem] * 8,
        [pltpu.VMEM((group_rows * block, LANES), f32)],
        8,
        BIG,
        "queries",
    )(
        table,
        tokens,
        norm_gains,
        w_query,
        w_key_up,
        w_query_rope,
        w_latent_down,
        w_rope_down.T,
    )
    received = lax.all_to_all(send, "tp", split_axis=0, concat_axis=0, tiled=True)
    send, latent_rows = kernel_call(
        functools.partial(attend_kernel, score_scale=(nope + rope) ** (-0.5)),
        (shape((tp_size, base, LANES), bf16), shape((per_head, LANES), f32)),
        [smem] + [vmem] * 6,
        [
            pltpu.VMEM((tp_size * base, LANES), f32),
            pltpu.VMEM((tp_size * 8, LANES), f32),
            pltpu.VMEM((heads, LANES), f32),
            pltpu.VMEM((heads, latent), bf16),
        ],
        8,
        4 * heads * cached * latent,
        "attend",
    )(
        lengths,
        received,
        cache_latent[0],
        cache_rope[0].T,
        table,
        latent_gain.reshape(-1, LANES),
        rope_row,
    )
    received = lax.all_to_all(send, "tp", split_axis=0, concat_axis=0, tiled=True)
    everyone = ("ep", "tp")

    def swap(value):
        return lax.ppermute(value, "tp", [(i, i ^ 1) for i in range(tp_size)])

    def plane(value, low, high):
        pairs = [(i, i ^ (2 * (high if i % 2 else low)) ^ 1) for i in range(tp_size)]
        return lax.ppermute(value, "tp", pairs)

    def along(value, low, high):
        pairs = [(i, i ^ (tp_size * (high if i % 2 else low)) ^ 1) for i in range(devices)]
        return lax.ppermute(value, everyone, pairs)

    send = kernel_call(
        output_kernel,
        shape((tp_size, pieces, LANES), bf16),
        [vmem] * 3,
        [
            pltpu.VMEM((tp_size * base, LANES), f32),
            pltpu.VMEM((tp_size * pieces, LANES), f32),
        ],
        10,
        2 * group_rows * (w_output.size + w_value_up.size),
        "outputs",
    )(received, w_value_up, w_output)
    row_block = shape((tp_size, pieces, LANES), bf16)
    half_block = shape((chips, pieces, LANES), bf16)
    own, half = kernel_call(
        pair_half_kernel, (row_block, half_block), [vmem] * 2, [], 2, send.size, "pair_rows"
    )(send, swap(send))
    pairs, last = mask_pairs(chips)
    parts = [plane(own, low, high) for low, high in pairs] + [plane(half, last, last)]
    partial = kernel_call(
        combine_kernel, row_block, [vmem] * len(parts), [], 2, send.size, "combine"
    )(*parts)
    send, half, resid, scales = kernel_call(
        resid_kernel,
        (
            row_block,
            half_block,
            shape((pieces, LANES), f32),
            shape((ep_size, LANES), f32),
        ),
        [vmem] * 7,
        [pltpu.VMEM((tp_size, pieces, LANES), f32)],
        4,
        10 * tp_size * width,
        "resid",
    )(routes.T, route_weights.T, token_rows, gain_rows, own, partial, swap(partial))
    masks = mask_pairs(ep_size)
    pairs, last = masks
    parts = [along(send, low, high) for low, high in pairs] + [along(half, last, last)]
    joined = len(pairs) * tp_size + chips
    mine = kernel_call(
        join_kernel,
        shape((joined, pieces, LANES), bf16),
        [vmem] * len(parts),
        [],
        2,
        send.size,
        "join",
    )(*parts)
    others = swap(mine)
    half = pieces // 2
    keep, give = kernel_call(
        functools.partial(expert_kernel, masks=masks),
        (shape((devices, half, LANES), f32), shape((devices, half, LANES), bf16)),
        [vmem] * 6,
        [
            pltpu.VMEM((devices * pieces, LANES), f32),
            pltpu.VMEM((devices, width), bf16),
        ],
        12,
        6 * devices * w_gate.size,
        "experts",
    )(send, mine, others, w_gate[0], w_up[0], w_down[0])
    got = swap(give)
    send = kernel_call(
        pair_kernel,
        shape((devices, half, LANES), bf16),
        [vmem] * 2,
        [],
        4,
        give.size,
        "pair_columns",
    )(keep, got)
    received = lax.all_to_all(send, everyone, split_axis=0, concat_axis=0, tiled=True)
    return kernel_call(
        final_kernel,
        (shape((1, width), bf16), shape((1, latent), bf16), shape((1, rope), bf16)),
        [vmem] * 6,
        [],
        4,
        2 * devices * width,
        "final",
    )(scales, received, resid, gain_rows, latent_rows, rope_row)


def on_device(*arrays):
    w_key_up, w_value_up, w_latent_down, w_rope_down = (arrays[i] for i in (4, 5, 7, 9))
    if lanes_fit(
        w_key_up, w_value_up, w_latent_down, w_rope_down, arrays[10], lax.axis_size("tp")
    ):
        return on_device_fused(*arrays)
    return on_device_plain(*arrays)


def solution(mesh):
    in_specs = (
        P("ep", None),
        P(),
        P(None, "tp"),
        P(None, "tp"),
        P("tp", None, None),
        P("tp", None, None),
        P("tp", None),
        P(None, "tp"),
        P(),
        P(),
        P(("ep", "tp"), None, None),
        P(("ep", "tp"), None, None),
        P(("ep", "tp")),
        P("ep", None),
        P("ep", None),
        P("ep", None, "tp"),
        P("ep", None, "tp"),
        P("ep", "tp", None),
    )
    out_specs = (P(("ep", "tp"), None), P(("ep", "tp"), None), P(("ep", "tp"), None))
    return jax.shard_map(
        on_device, mesh=mesh, in_specs=in_specs, out_specs=out_specs, check_vma=False
    )
```

```python
import functools
import math

import jax
import jax.numpy as jnp
from jax import lax
from jax.experimental import pallas as pl
from jax.experimental.pallas import tpu as pltpu
from jax.sharding import PartitionSpec as P

EPSILON = 1e-06
ROTARY_BASE = 500000.0


def rms_scale(source, gain_row):
    values_f = source.astype(jnp.float32)
    return (
        values_f
        * lax.rsqrt(jnp.mean(values_f * values_f, axis=-1, keepdims=True) + EPSILON)
        * gain_row
    )


def rotate(source, position):
    half_width = source.shape[-1] // 2
    frequency = ROTARY_BASE ** (-jnp.arange(half_width, dtype=jnp.float32) / half_width)
    angles = position[..., None] * frequency
    first_half = source[..., :half_width]
    second_half = source[..., half_width:]
    return jnp.concatenate(
        [
            first_half * jnp.cos(angles) - second_half * jnp.sin(angles),
            second_half * jnp.cos(angles) + first_half * jnp.sin(angles),
        ],
        axis=-1,
    )


def attend(q_latent, q_pe, cache_lat, cache_rp, lat_new, rope_new, lengths, score_scale):
    scores = (
        jnp.einsum("shc,spc->shp", q_latent, cache_lat, preferred_element_type=jnp.float32)
        + jnp.einsum("shr,spr->shp", q_pe, cache_rp, preferred_element_type=jnp.float32)
    ) * score_scale
    own_score = (
        jnp.einsum("shc,sc->sh", q_latent, lat_new, preferred_element_type=jnp.float32)
        + jnp.einsum("shr,sr->sh", q_pe, rope_new, preferred_element_type=jnp.float32)
    ) * score_scale
    visible = (
        jnp.arange(cache_lat.shape[1], dtype=jnp.int32)[None, None, :] < lengths[:, None, None]
    )
    row_max = jnp.maximum(jnp.max(jnp.where(visible, scores, -jnp.inf), axis=-1), own_score)
    weights = jnp.where(visible, jnp.exp(scores - row_max[..., None]), 0.0)
    own_weight = jnp.exp(own_score - row_max)
    denominator = jnp.sum(weights, axis=-1) + own_weight
    probabilities = (weights / denominator[..., None]).astype(jnp.bfloat16)
    own_prob = (own_weight / denominator).astype(jnp.bfloat16)
    attended = jnp.einsum(
        "shp,spc->shc", probabilities, cache_lat, preferred_element_type=jnp.float32
    )
    attended = (
        attended + own_prob.astype(jnp.float32)[..., None] * lat_new.astype(jnp.float32)[:, None, :]
    )
    return attended.astype(jnp.bfloat16)


def to_sequences(rows, tp_size, seq_count):
    blocks = rows.reshape(tp_size, seq_count, rows.shape[1])
    return lax.all_to_all(blocks, "tp", split_axis=0, concat_axis=0, tiled=True)


def on_device_plain(
    tokens,
    norm_gains,
    w_query,
    w_query_rope,
    w_key_up,
    w_value_up,
    w_output,
    w_latent_down,
    latent_gain,
    w_rope_down,
    cache_latent,
    cache_rope,
    lengths,
    routes,
    route_weights,
    w_gate,
    w_up,
    w_down,
):
    group_rows = tokens.shape[0]
    seq_count = cache_latent.shape[0]
    heads_here = w_key_up.shape[0]
    nope_width = w_key_up.shape[1]
    rope_width = w_rope_down.shape[1]
    tp_size = lax.axis_size("tp")
    tp_rank = lax.axis_index("tp")
    normed = rms_scale(tokens, norm_gains[0]).astype(jnp.bfloat16)
    q_nope = jnp.dot(normed, w_query, preferred_element_type=jnp.float32).astype(jnp.bfloat16)
    q_nope = q_nope.reshape(group_rows, heads_here, nope_width)
    q_latent = jnp.einsum("thn,hnc->thc", q_nope, w_key_up, preferred_element_type=jnp.float32)
    q_latent = q_latent.astype(jnp.bfloat16).reshape(group_rows, -1)
    q_rot = jnp.dot(normed, w_query_rope, preferred_element_type=jnp.float32).astype(jnp.bfloat16)
    latent_cols = jnp.dot(normed, w_latent_down, preferred_element_type=jnp.float32).astype(
        jnp.bfloat16
    )
    q_cols, rot_cols = q_latent.shape[1], q_rot.shape[1]
    packed = jnp.concatenate([q_latent, q_rot, latent_cols], axis=1)
    packed = to_sequences(packed, tp_size, seq_count)
    q_mine = packed[:, :, :q_cols].transpose(1, 0, 2).reshape(seq_count, -1)
    rot_mine = packed[:, :, q_cols : q_cols + rot_cols].transpose(1, 0, 2).reshape(seq_count, -1)
    latent_raw = packed[:, :, q_cols + rot_cols :].transpose(1, 0, 2).reshape(seq_count, -1)
    heads_all = rot_mine.shape[1] // rope_width
    own_normed = lax.dynamic_slice_in_dim(normed, tp_rank * seq_count, seq_count, 0)
    rope_raw = jnp.dot(own_normed, w_rope_down, preferred_element_type=jnp.float32).astype(
        jnp.bfloat16
    )
    new_latent = rms_scale(latent_raw, latent_gain).astype(jnp.bfloat16)
    position = lengths.astype(jnp.float32)
    new_rope = rotate(rope_raw.astype(jnp.float32), position).astype(jnp.bfloat16)
    q_pe = rotate(
        rot_mine.reshape(seq_count, heads_all, rope_width).astype(jnp.float32), position[:, None]
    )
    q_pe = q_pe.astype(jnp.bfloat16)
    score_scale = (nope_width + rope_width) ** (-0.5)
    attended = attend(
        q_mine.reshape(seq_count, heads_all, -1),
        q_pe,
        cache_latent,
        cache_rope,
        new_latent,
        new_rope,
        lengths,
        score_scale,
    )
    head_latent = lax.all_to_all(
        attended.reshape(seq_count, -1), "tp", split_axis=1, concat_axis=0, tiled=True
    )
    values = (
        jnp.einsum(
            "thc,hcv->thv",
            head_latent.reshape(group_rows, heads_here, -1),
            w_value_up,
            preferred_element_type=jnp.float32,
        )
        .astype(jnp.bfloat16)
        .reshape(group_rows, -1)
    )
    head_term = jnp.dot(values, w_output, preferred_element_type=jnp.float32)
    terms = to_sequences(head_term.astype(jnp.bfloat16), tp_size, seq_count)
    mixed = jnp.sum(terms.astype(jnp.float32), axis=0)
    own_tokens = lax.dynamic_slice_in_dim(tokens, tp_rank * seq_count, seq_count, 0)
    own_resid = (own_tokens.astype(jnp.float32) + rms_scale(mixed, norm_gains[1])).astype(
        jnp.bfloat16
    )
    expert_in = rms_scale(own_resid, norm_gains[2]).astype(jnp.bfloat16)
    everyone = ("ep", "tp")
    devices = lax.axis_size("ep") * tp_size
    copies = jnp.broadcast_to(expert_in[None], (devices,) + expert_in.shape)
    arrived = lax.all_to_all(copies, everyone, split_axis=0, concat_axis=0, tiled=True)
    arrived = arrived.reshape(devices * seq_count, -1)
    gate_sum = jnp.dot(arrived, w_gate[0], preferred_element_type=jnp.float32)
    up_sum = jnp.dot(arrived, w_up[0], preferred_element_type=jnp.float32)
    hidden_units = (jax.nn.silu(gate_sum) * up_sum).astype(jnp.bfloat16)
    pieces = jnp.dot(hidden_units, w_down[0], preferred_element_type=jnp.float32).astype(
        jnp.bfloat16
    )
    pieces = pieces.reshape(devices, seq_count, -1)
    returned = lax.all_to_all(pieces, everyone, split_axis=0, concat_axis=0, tiled=True)
    own_routes = lax.dynamic_slice_in_dim(routes, tp_rank * seq_count, seq_count, 0)
    own_weights = lax.dynamic_slice_in_dim(route_weights, tp_rank * seq_count, seq_count, 0)
    holder = jnp.arange(devices, dtype=jnp.int32) // tp_size
    picks = own_routes[None, :, :] == holder[:, None, None]
    scale = jnp.sum(jnp.where(picks, own_weights[None], 0.0), axis=-1)
    routed = jnp.sum(scale[:, :, None] * returned.astype(jnp.float32), axis=0)
    hidden_out = (own_resid.astype(jnp.float32) + rms_scale(routed, norm_gains[3])).astype(
        jnp.bfloat16
    )
    return (hidden_out, new_latent, new_rope)


LANES = 128
BIG = 20 * 10**9


def lane_chunk(value, index):
    return value[:, index * LANES : (index + 1) * LANES]


def mean_scale(value, count):
    return lax.rsqrt(jnp.sum(value * value, keepdims=True) / count + EPSILON)


def angle_kernel(lengths, table):
    half = LANES // 2
    lane = lax.broadcasted_iota(jnp.int32, (1, LANES), 1)
    exponent = (lane % (half // 2)).astype(jnp.float32) * (-math.log(ROTARY_BASE) / (half // 2))
    angles = lengths[0].astype(jnp.float32) * jnp.exp(exponent)
    sine = jnp.sin(angles)
    table[0:1, :] = jnp.cos(angles)
    table[1:2, :] = jnp.where(lane % half < half // 2, -sine, sine)


def tail_kernel(
    table,
    tokens,
    gains,
    w_query_rope,
    w_latent,
    w_rope,
    normed_rows,
    tail_rows,
    rope_row,
    token_rows,
    gain_rows,
):
    group_rows, width = tokens.shape
    pieces = width // LANES
    heads = w_query_rope.shape[1] * 2 // LANES
    tail = tail_rows.shape[0] // group_rows
    tokens_f = tokens[...].astype(jnp.float32)
    power = jnp.sum(tokens_f * tokens_f, axis=-1, keepdims=True) / width
    normed = (tokens_f * lax.rsqrt(power + EPSILON) * gains[0:1, :]).astype(jnp.bfloat16)
    normed_rows[...] = normed
    q_rot = jnp.dot(normed, w_query_rope[...], preferred_element_type=jnp.float32)
    latent_cols = jnp.dot(normed, w_latent[...], preferred_element_type=jnp.float32)
    rope_raw = lax.dot_general(
        normed, w_rope[...], (((1,), (1,)), ((), ())), preferred_element_type=jnp.float32
    )
    half = LANES // 2
    low = lax.broadcasted_iota(jnp.int32, (group_rows, LANES), 1) < half
    for h in range(heads):
        pair = lane_chunk(q_rot, h // 2)
        turned = pltpu.roll(pair, half, 1)
        twice = jnp.where(low, pair, turned) if h % 2 == 0 else jnp.where(low, turned, pair)
        tail_rows[pl.ds(h, group_rows, stride=tail), :] = twice
    for k in range(heads, tail):
        tail_rows[pl.ds(k, group_rows, stride=tail), :] = latent_cols
    for k in range(pieces):
        token_rows[pl.ds(k, group_rows, stride=pieces), :] = lane_chunk(tokens_f, k)
        gain_rows[pl.ds(k, gains.shape[0], stride=pieces), :] = lane_chunk(gains[...], k)
    mine = lax.broadcasted_iota(jnp.int32, rope_raw.shape, 0) == lax.axis_index("tp")
    rope_raw = jnp.sum(jnp.where(mine, rope_raw, 0.0), axis=0, keepdims=True)
    rope_raw = rope_raw.astype(jnp.bfloat16).astype(jnp.float32)
    twice = jnp.concatenate([rope_raw, rope_raw], axis=1)
    turned = twice * table[0:1, :] + pltpu.roll(twice, half // 2, 1) * table[1:2, :]
    rope_row[...] = turned.astype(jnp.bfloat16).astype(jnp.float32)


def query_kernel(normed, tail_rows, w_query, w_key, send, rows):
    group_rows = normed.shape[0]
    heads, nope, latent = w_key.shape
    per_head = latent // LANES
    base = heads * per_head
    tail = tail_rows.shape[0] // group_rows
    q_nope = jnp.dot(normed[...], w_query[...], preferred_element_type=jnp.float32)
    q_nope = q_nope.astype(jnp.bfloat16)
    for h in range(heads):
        q_latent = jnp.dot(
            q_nope[:, h * nope : (h + 1) * nope], w_key[h], preferred_element_type=jnp.float32
        )
        for k in range(per_head):
            rows[pl.ds(h * per_head + k, group_rows, stride=base), :] = lane_chunk(q_latent, k)
    for j in range(group_rows):
        send[j, :base] = rows[pl.ds(j * base, base), :].astype(jnp.bfloat16)
        send[j, base:] = tail_rows[pl.ds(j * tail, tail), :].astype(jnp.bfloat16)


def attend_kernel(
    length,
    received,
    cache,
    cache_rope,
    table,
    gain,
    rope_row,
    send,
    latent_rows,
    rows,
    extra,
    rot_rows,
    queries,
    score_scale,
):
    sources, block, _ = received.shape
    latent = cache.shape[1]
    per_head = latent // LANES
    rope = cache_rope.shape[0]
    heads = queries.shape[0]
    here = heads // sources
    base = here * per_head
    tail = block - base
    for j in range(sources):
        piece = received[j].astype(jnp.float32)
        rows[pl.ds(j * base, base), :] = piece[:base]
        extra[pl.ds(j * tail, tail), :] = piece[base:]
    for k in range(per_head):
        queries[:, k * LANES : (k + 1) * LANES] = rows[
            pl.ds(k, heads, stride=per_head), :
        ].astype(jnp.bfloat16)
    for j in range(sources):
        rot_rows[pl.ds(j * here, here), :] = extra[pl.ds(j * tail, here), :]
    latent_raw = extra[pl.ds(here, sources, stride=tail), :]
    latent_f = (latent_raw * mean_scale(latent_raw, latent) * gain[...]).astype(jnp.bfloat16)
    latent_f = latent_f.astype(jnp.float32)
    latent_rows[...] = latent_f
    rot = rot_rows[...]
    q_pe = rot * table[0:1, :] + pltpu.roll(rot, LANES // 4, 1) * table[1:2, :]
    q_pe = q_pe[:, :rope].astype(jnp.bfloat16)
    q = queries[...]
    scores = lax.dot_general(
        q, cache[...], (((1,), (1,)), ((), ())), preferred_element_type=jnp.float32
    )
    scores = scores + jnp.dot(q_pe, cache_rope[...], preferred_element_type=jnp.float32)
    scores = scores * score_scale
    q_f = q.astype(jnp.float32)
    products = lane_chunk(q_f, 0) * latent_f[0:1, :]
    for k in range(1, per_head):
        products = products + lane_chunk(q_f, k) * latent_f[k : k + 1, :]
    own = jnp.sum(products, axis=1, keepdims=True)
    own = own + jnp.sum(
        q_pe.astype(jnp.float32) * rope_row[:, :rope], axis=1, keepdims=True
    )
    own = own * score_scale
    visible = lax.broadcasted_iota(jnp.int32, scores.shape, 1) < length[0]
    top = jnp.maximum(jnp.max(jnp.where(visible, scores, -jnp.inf), axis=1, keepdims=True), own)
    weights = jnp.where(visible, jnp.exp(scores - top), 0.0)
    own_weight = jnp.exp(own - top)
    total = jnp.sum(weights, axis=1, keepdims=True) + own_weight
    probs = (weights / total).astype(jnp.bfloat16)
    own_prob = (own_weight / total).astype(jnp.bfloat16).astype(jnp.float32)
    attended = jnp.dot(probs, cache[...], preferred_element_type=jnp.float32)
    for k in range(per_head):
        rows[pl.ds(k, heads, stride=per_head), :] = (
            lane_chunk(attended, k) + own_prob * latent_f[k : k + 1, :]
        )
    for j in range(sources):
        send[j] = rows[pl.ds(j * base, base), :].astype(jnp.bfloat16)


def output_kernel(received, w_value, w_output, send, rows, term_rows):
    sources, block, _ = received.shape
    heads, latent, _ = w_value.shape
    per_head = latent // LANES
    pieces = w_output.shape[1] // LANES
    for j in range(sources):
        rows[pl.ds(j * block, block), :] = received[j].astype(jnp.float32)
    values = []
    for h in range(heads):
        attended = jnp.concatenate(
            [
                rows[pl.ds(h * per_head + k, sources, stride=block), :].astype(jnp.bfloat16)
                for k in range(per_head)
            ],
            axis=1,
        )
        values.append(
            jnp.dot(attended, w_value[h], preferred_element_type=jnp.float32).astype(jnp.bfloat16)
        )
    values = jnp.concatenate(values, axis=1)
    step = 4
    for c in range(0, pieces, step):
        term = jnp.dot(
            values,
            w_output[:, c * LANES : (c + step) * LANES],
            preferred_element_type=jnp.float32,
        )
        for k in range(step):
            term_rows[pl.ds(c + k, sources, stride=pieces), :] = lane_chunk(term, k)
    for j in range(sources):
        send[j] = term_rows[pl.ds(j * pieces, pieces), :].astype(jnp.bfloat16)


def half_rows(core, count):
    return [core * count + i for i in range(count)]


def pair_kernel(keep, got, send):
    for i in range(send.shape[0]):
        total = keep[i].astype(jnp.float32) + got[i].astype(jnp.float32)
        send[i] = total.astype(jnp.bfloat16)


def pair_half_kernel(keep, got, send, half):
    pair_kernel(keep, got, send)
    for i, row in enumerate(half_rows(lax.axis_index("tp") % 2, half.shape[0])):
        half[i] = send[row]


def combine_kernel(*refs):
    full, half, total = refs[:-2], refs[-2], refs[-1]
    for i in range(total.shape[0]):
        value = jnp.zeros(total.shape[1:], jnp.float32)
        for ref in full:
            value = value + ref[i].astype(jnp.float32)
        total[i] = value.astype(jnp.bfloat16)
    for i, row in enumerate(half_rows(1 - lax.axis_index("tp") % 2, half.shape[0])):
        value = half[i].astype(jnp.float32)
        for ref in full:
            value = value + ref[row].astype(jnp.float32)
        total[row] = value.astype(jnp.bfloat16)


def join_kernel(*refs):
    joined = refs[-1]
    place = 0
    for ref in refs[:-1]:
        for i in range(ref.shape[0]):
            joined[place + i] = ref[i]
        place += ref.shape[0]


def row_scales(blocks, count):
    power = [jnp.sum(block * block, axis=0, keepdims=True) for block in blocks]
    power = jnp.sum(jnp.concatenate(power, axis=0), axis=1, keepdims=True) / count
    scale = lax.rsqrt(power + EPSILON)
    return [scale[i : i + 1, :] for i in range(len(blocks))]


def resid_kernel(
    routes,
    route_weights,
    token_rows,
    gain_rows,
    own,
    partial,
    got,
    send,
    half,
    resid,
    scales,
    after_rows,
):
    rank = lax.axis_index("tp")
    mine = lax.broadcasted_iota(jnp.int32, routes.shape, 1) == rank
    named = jnp.sum(jnp.where(mine, routes[...], 0), axis=1, keepdims=True)
    weight = jnp.sum(jnp.where(mine, route_weights[...], 0.0), axis=1, keepdims=True)
    for e in range(scales.shape[0]):
        total = jnp.sum(jnp.where(named == e, weight, 0.0), axis=0, keepdims=True)
        scales[e : e + 1, :] = jnp.broadcast_to(total, (1, LANES))
    count, pieces, _ = send.shape
    width = pieces * LANES
    mixed = [
        own[i].astype(jnp.float32)
        + (partial[i].astype(jnp.float32) + got[i].astype(jnp.float32))
        for i in range(count)
    ]
    gain = gain_rows[pieces : 2 * pieces, :]
    after = [
        (token_rows[i * pieces : (i + 1) * pieces, :] + mixed[i] * scale * gain)
        .astype(jnp.bfloat16)
        .astype(jnp.float32)
        for i, scale in enumerate(row_scales(mixed, width))
    ]
    gain = gain_rows[2 * pieces : 3 * pieces, :]
    for i, scale in enumerate(row_scales(after, width)):
        after_rows[i] = after[i]
        send[i] = (after[i] * scale * gain).astype(jnp.bfloat16)
    resid[...] = after_rows[rank]
    for i, row in enumerate(half_rows(rank % 2, half.shape[0])):
        half[i] = send[row]


def expert_kernel(*refs):
    parts, (w_gate, w_up, w_down, keep, give, rows, inputs) = refs[:-7], refs[-7:]
    blocks = [part[i] for part in parts for i in range(part.shape[0])]
    count = len(blocks)
    pieces = blocks[0].shape[0]
    for i, block in enumerate(blocks):
        rows[pl.ds(i * pieces, pieces), :] = block.astype(jnp.float32)
    for k in range(pieces):
        inputs[:, k * LANES : (k + 1) * LANES] = rows[
            pl.ds(k, count, stride=pieces), :
        ].astype(jnp.bfloat16)
    gate = jnp.dot(inputs[...], w_gate[...], preferred_element_type=jnp.float32)
    up = jnp.dot(inputs[...], w_up[...], preferred_element_type=jnp.float32)
    inner = (gate / (1.0 + jnp.exp(-gate)) * up).astype(jnp.bfloat16)
    step = 4
    for k in range(0, pieces, step):
        piece = jnp.dot(
            inner, w_down[:, k * LANES : (k + step) * LANES], preferred_element_type=jnp.float32
        )
        piece = piece.astype(jnp.bfloat16).astype(jnp.float32)
        for j in range(step):
            rows[pl.ds(k + j, count, stride=pieces), :] = lane_chunk(piece, j)
    core = lax.axis_index("tp") % 2
    half = pieces // 2
    for i in range(count):
        start = pl.multiple_of(i * pieces + core * half, half)
        keep[i] = rows[pl.ds(start, half), :]
        start = pl.multiple_of(i * pieces + (1 - core) * half, half)
        give[i] = rows[pl.ds(start, half), :].astype(jnp.bfloat16)


def place_kernel(own, mine, others, got_early, got_late, send, masks):
    members = own.shape[0]
    core = lax.axis_index("tp") % 2
    group = lax.axis_index("ep")
    pairs, last = masks

    def places(side):
        listed = []
        for low, high in pairs:
            other = group ^ jnp.where(side == 0, low, high)
            listed += [other * members + i for i in range(members)]
        return listed + [(group ^ last) * members + row for row in half_rows(side, members // 2)]

    def put(place, kept, got):
        send[place] = (kept + got.astype(jnp.float32)).astype(jnp.bfloat16)

    for i in range(members):
        put(group * members + i, own[i], got_early[i])
    for i, place in enumerate(places(1 - core)):
        put(place, mine[i], got_late[i])
    for i, place in enumerate(places(core)):
        put(place, others[i], got_early[members + i])


def final_kernel(
    scales, received, resid, gain_rows, latent_rows, rope_row, hidden, new_latent, new_rope
):
    for k in range(latent_rows.shape[0]):
        new_latent[:, k * LANES : (k + 1) * LANES] = latent_rows[k : k + 1, :].astype(
            jnp.bfloat16
        )
    new_rope[...] = rope_row[:, : new_rope.shape[1]].astype(jnp.bfloat16)
    sources, half, _ = received.shape
    pieces = 2 * half
    experts = scales.shape[0]
    per_expert = sources // experts
    parts = []
    for c in range(2):
        total = None
        for e in range(experts):
            block = received[e * per_expert + c].astype(jnp.float32)
            for b in range(c + 2, per_expert, 2):
                block = block + received[e * per_expert + b].astype(jnp.float32)
            part = block * scales[e : e + 1, :]
            total = part if total is None else total + part
        parts.append(total)
    routed = jnp.concatenate(parts, axis=0)
    out = resid[...] + routed * mean_scale(routed, pieces * LANES) * gain_rows[3 * pieces :]
    for k in range(pieces):
        hidden[:, k * LANES : (k + 1) * LANES] = out[k : k + 1, :].astype(jnp.bfloat16)


def kernel_call(body, outs, specs, scratch, megabytes, flops, name):
    bytes_moved = flops // BIG * 32 * 1024 * 1024 if flops >= BIG else min(flops, 4 * 1024 * 1024)
    return pl.pallas_call(
        body,
        out_shape=outs,
        in_specs=specs,
        out_specs=jax.tree.map(lambda _: pl.BlockSpec(memory_space=pltpu.VMEM), outs),
        scratch_shapes=scratch,
        compiler_params=pltpu.CompilerParams(vmem_limit_bytes=megabytes * 1024 * 1024),
        cost_estimate=pl.CostEstimate(
            flops=flops, bytes_accessed=bytes_moved, transcendentals=0
        ),
        name=name,
    )


def mask_pairs(size):
    return [(m, m - 1) for m in range(size - 1, 1, -2)], 1


def far_half_pairs(size):
    return [(m, m + 1) for m in range(1, size - 1, 2)], size - 1


def power_of_two(size):
    return size & (size - 1) == 0


def lanes_fit(w_key_up, w_value_up, w_latent_down, w_rope_down, cache_latent, tp_size):
    return (
        cache_latent.shape[0] == 1
        and power_of_two(tp_size)
        and power_of_two(lax.axis_size("ep"))
        and tp_size > 2
        and lax.axis_size("ep") > 1
        and w_latent_down.shape[1] == LANES
        and w_key_up.shape[0] % 2 == 0
        and w_key_up.shape[1] == LANES
        and w_value_up.shape[2] == LANES
        and 2 * w_rope_down.shape[1] == LANES
        and w_key_up.shape[2] == tp_size * LANES
        and w_key_up.shape[0] * w_key_up.shape[2] // LANES % 8 == 0
        and w_key_up.shape[0] < 8
    )


def on_device_fused(
    tokens,
    norm_gains,
    w_query,
    w_query_rope,
    w_key_up,
    w_value_up,
    w_output,
    w_latent_down,
    latent_gain,
    w_rope_down,
    cache_latent,
    cache_rope,
    lengths,
    routes,
    route_weights,
    w_gate,
    w_up,
    w_down,
):
    tp_size = lax.axis_size("tp")
    ep_size = lax.axis_size("ep")
    devices = tp_size * ep_size
    heads_here, nope, latent = w_key_up.shape
    heads = heads_here * tp_size
    chips = tp_size // 2
    group_rows, width = tokens.shape
    rope = w_rope_down.shape[1]
    cached = cache_latent.shape[1]
    pieces = width // LANES
    per_head = latent // LANES
    base = heads_here * per_head
    block = base + 8
    bf16, f32 = jnp.bfloat16, jnp.float32
    vmem = pl.BlockSpec(memory_space=pltpu.VMEM)
    smem = pl.BlockSpec(memory_space=pltpu.SMEM)
    shape = jax.ShapeDtypeStruct

    table = kernel_call(
        angle_kernel, shape((2, LANES), f32), [smem], [], 1, 2 * BIG, "angles"
    )(lengths)
    normed, tail_rows, rope_row, token_rows, gain_rows = kernel_call(
        tail_kernel,
        (
            shape((group_rows, width), bf16),
            shape((group_rows * 8, LANES), f32),
            shape((1, LANES), f32),
            shape((group_rows * pieces, LANES), f32),
            shape((norm_gains.shape[0] * pieces, LANES), f32),
        ),
        [vmem] * 6,
        [],
        6,
        1,
        "tails",
    )(table, tokens, norm_gains, w_query_rope, w_latent_down, w_rope_down.T)
    send = kernel_call(
        query_kernel,
        shape((tp_size, block, LANES), bf16),
        [vmem] * 4,
        [pltpu.VMEM((group_rows * base, LANES), f32)],
        6,
        BIG,
        "queries",
    )(normed, tail_rows, w_query, w_key_up)
    received = lax.all_to_all(send, "tp", split_axis=0, concat_axis=0, tiled=True)
    send, latent_rows = kernel_call(
        functools.partial(attend_kernel, score_scale=(nope + rope) ** (-0.5)),
        (shape((tp_size, base, LANES), bf16), shape((per_head, LANES), f32)),
        [smem] + [vmem] * 6,
        [
            pltpu.VMEM((tp_size * base, LANES), f32),
            pltpu.VMEM((tp_size * 8, LANES), f32),
            pltpu.VMEM((heads, LANES), f32),
            pltpu.VMEM((heads, latent), bf16),
        ],
        8,
        4 * heads * cached * latent,
        "attend",
    )(
        lengths,
        received,
        cache_latent[0],
        cache_rope[0].T,
        table,
        latent_gain.reshape(-1, LANES),
        rope_row,
    )
    received = lax.all_to_all(send, "tp", split_axis=0, concat_axis=0, tiled=True)
    everyone = ("ep", "tp")

    def swap(value):
        return lax.ppermute(value, "tp", [(i, i ^ 1) for i in range(tp_size)])

    def plane(value, low, high):
        pairs = [(i, i ^ (2 * (high if i % 2 else low)) ^ 1) for i in range(tp_size)]
        return lax.ppermute(value, "tp", pairs)

    def along(value, low, high):
        pairs = [(i, i ^ (tp_size * (high if i % 2 else low)) ^ 1) for i in range(devices)]
        return lax.ppermute(value, everyone, pairs)

    send = kernel_call(
        output_kernel,
        shape((tp_size, pieces, LANES), bf16),
        [vmem] * 3,
        [
            pltpu.VMEM((tp_size * base, LANES), f32),
            pltpu.VMEM((tp_size * pieces, LANES), f32),
        ],
        10,
        2 * group_rows * (w_output.size + w_value_up.size),
        "outputs",
    )(received, w_value_up, w_output)
    row_block = shape((tp_size, pieces, LANES), bf16)
    half_block = shape((chips, pieces, LANES), bf16)
    own, half = kernel_call(
        pair_half_kernel, (row_block, half_block), [vmem] * 2, [], 2, send.size, "pair_rows"
    )(send, swap(send))
    pairs, last = mask_pairs(chips)
    parts = [plane(own, low, high) for low, high in pairs] + [plane(half, last, last)]
    partial = kernel_call(
        combine_kernel, row_block, [vmem] * len(parts), [], 2, send.size, "combine"
    )(*parts)
    send, half, resid, scales = kernel_call(
        resid_kernel,
        (
            row_block,
            half_block,
            shape((pieces, LANES), f32),
            shape((ep_size, LANES), f32),
        ),
        [vmem] * 7,
        [pltpu.VMEM((tp_size, pieces, LANES), f32)],
        4,
        10 * tp_size * width,
        "resid",
    )(routes.T, route_weights.T, token_rows, gain_rows, own, partial, swap(partial))
    masks = far_half_pairs(ep_size)
    pairs, last = masks
    parts = [along(send, low, high) for low, high in pairs] + [along(half, last, last)]
    joined = len(pairs) * tp_size + chips
    mine = kernel_call(
        join_kernel,
        shape((joined, pieces, LANES), bf16),
        [vmem] * len(parts),
        [],
        2,
        send.size,
        "join",
    )(*parts)
    others = swap(mine)
    half = pieces // 2

    def run_experts(parts, name):
        count = sum(part.shape[0] for part in parts)
        return kernel_call(
            expert_kernel,
            (shape((count, half, LANES), f32), shape((count, half, LANES), bf16)),
            [vmem] * (len(parts) + 3),
            [pltpu.VMEM((count * pieces, LANES), f32), pltpu.VMEM((count, width), bf16)],
            8,
            2 * 10**9,
            name,
        )(*parts, w_gate[0], w_up[0], w_down[0])

    own_keep, own_give = run_experts([send], "experts_own")
    mine_keep, mine_give = run_experts(parts, "experts_mine")
    early = kernel_call(
        join_kernel,
        shape((tp_size + joined, half, LANES), bf16),
        [vmem] * 2,
        [],
        2,
        send.size,
        "join_early",
    )(own_give, mine_give)
    got_early = swap(early)
    others_keep, others_give = run_experts([others], "experts_others")
    send = kernel_call(
        functools.partial(place_kernel, masks=masks),
        shape((devices, half, LANES), bf16),
        [vmem] * 5,
        [],
        4,
        send.size,
        "place",
    )(own_keep, mine_keep, others_keep, got_early, swap(others_give))
    received = lax.all_to_all(send, everyone, split_axis=0, concat_axis=0, tiled=True)
    return kernel_call(
        final_kernel,
        (shape((1, width), bf16), shape((1, latent), bf16), shape((1, rope), bf16)),
        [vmem] * 6,
        [],
        4,
        2 * devices * width,
        "final",
    )(scales, received, resid, gain_rows, latent_rows, rope_row)


def on_device(*arrays):
    w_key_up, w_value_up, w_latent_down, w_rope_down = (arrays[i] for i in (4, 5, 7, 9))
    if lanes_fit(
        w_key_up, w_value_up, w_latent_down, w_rope_down, arrays[10], lax.axis_size("tp")
    ):
        return on_device_fused(*arrays)
    return on_device_plain(*arrays)


def solution(mesh):
    in_specs = (
        P("ep", None),
        P(),
        P(None, "tp"),
        P(None, "tp"),
        P("tp", None, None),
        P("tp", None, None),
        P("tp", None),
        P(None, "tp"),
        P(),
        P(),
        P(("ep", "tp"), None, None),
        P(("ep", "tp"), None, None),
        P(("ep", "tp")),
        P("ep", None),
        P("ep", None),
        P("ep", None, "tp"),
        P("ep", None, "tp"),
        P("ep", "tp", None),
    )
    out_specs = (P(("ep", "tp"), None), P(("ep", "tp"), None), P(("ep", "tp"), None))
    return jax.shard_map(
        on_device, mesh=mesh, in_specs=in_specs, out_specs=out_specs, check_vma=False
    )
```

```python
import functools
import math

import jax
import jax.numpy as jnp
from jax import lax
from jax.experimental import pallas as pl
from jax.experimental.pallas import tpu as pltpu
from jax.sharding import PartitionSpec as P

EPSILON = 1e-06
ROTARY_BASE = 500000.0


def rms_scale(source, gain_row):
    values_f = source.astype(jnp.float32)
    return (
        values_f
        * lax.rsqrt(jnp.mean(values_f * values_f, axis=-1, keepdims=True) + EPSILON)
        * gain_row
    )


def rotate(source, position):
    half_width = source.shape[-1] // 2
    frequency = ROTARY_BASE ** (-jnp.arange(half_width, dtype=jnp.float32) / half_width)
    angles = position[..., None] * frequency
    first_half = source[..., :half_width]
    second_half = source[..., half_width:]
    return jnp.concatenate(
        [
            first_half * jnp.cos(angles) - second_half * jnp.sin(angles),
            second_half * jnp.cos(angles) + first_half * jnp.sin(angles),
        ],
        axis=-1,
    )


def attend(q_latent, q_pe, cache_lat, cache_rp, lat_new, rope_new, lengths, score_scale):
    scores = (
        jnp.einsum("shc,spc->shp", q_latent, cache_lat, preferred_element_type=jnp.float32)
        + jnp.einsum("shr,spr->shp", q_pe, cache_rp, preferred_element_type=jnp.float32)
    ) * score_scale
    own_score = (
        jnp.einsum("shc,sc->sh", q_latent, lat_new, preferred_element_type=jnp.float32)
        + jnp.einsum("shr,sr->sh", q_pe, rope_new, preferred_element_type=jnp.float32)
    ) * score_scale
    visible = (
        jnp.arange(cache_lat.shape[1], dtype=jnp.int32)[None, None, :] < lengths[:, None, None]
    )
    row_max = jnp.maximum(jnp.max(jnp.where(visible, scores, -jnp.inf), axis=-1), own_score)
    weights = jnp.where(visible, jnp.exp(scores - row_max[..., None]), 0.0)
    own_weight = jnp.exp(own_score - row_max)
    denominator = jnp.sum(weights, axis=-1) + own_weight
    probabilities = (weights / denominator[..., None]).astype(jnp.bfloat16)
    own_prob = (own_weight / denominator).astype(jnp.bfloat16)
    attended = jnp.einsum(
        "shp,spc->shc", probabilities, cache_lat, preferred_element_type=jnp.float32
    )
    attended = (
        attended + own_prob.astype(jnp.float32)[..., None] * lat_new.astype(jnp.float32)[:, None, :]
    )
    return attended.astype(jnp.bfloat16)


def to_sequences(rows, tp_size, seq_count):
    blocks = rows.reshape(tp_size, seq_count, rows.shape[1])
    return lax.all_to_all(blocks, "tp", split_axis=0, concat_axis=0, tiled=True)


def on_device_plain(
    tokens,
    norm_gains,
    w_query,
    w_query_rope,
    w_key_up,
    w_value_up,
    w_output,
    w_latent_down,
    latent_gain,
    w_rope_down,
    cache_latent,
    cache_rope,
    lengths,
    routes,
    route_weights,
    w_gate,
    w_up,
    w_down,
):
    group_rows = tokens.shape[0]
    seq_count = cache_latent.shape[0]
    heads_here = w_key_up.shape[0]
    nope_width = w_key_up.shape[1]
    rope_width = w_rope_down.shape[1]
    tp_size = lax.axis_size("tp")
    tp_rank = lax.axis_index("tp")
    normed = rms_scale(tokens, norm_gains[0]).astype(jnp.bfloat16)
    q_nope = jnp.dot(normed, w_query, preferred_element_type=jnp.float32).astype(jnp.bfloat16)
    q_nope = q_nope.reshape(group_rows, heads_here, nope_width)
    q_latent = jnp.einsum("thn,hnc->thc", q_nope, w_key_up, preferred_element_type=jnp.float32)
    q_latent = q_latent.astype(jnp.bfloat16).reshape(group_rows, -1)
    q_rot = jnp.dot(normed, w_query_rope, preferred_element_type=jnp.float32).astype(jnp.bfloat16)
    latent_cols = jnp.dot(normed, w_latent_down, preferred_element_type=jnp.float32).astype(
        jnp.bfloat16
    )
    q_cols, rot_cols = q_latent.shape[1], q_rot.shape[1]
    packed = jnp.concatenate([q_latent, q_rot, latent_cols], axis=1)
    packed = to_sequences(packed, tp_size, seq_count)
    q_mine = packed[:, :, :q_cols].transpose(1, 0, 2).reshape(seq_count, -1)
    rot_mine = packed[:, :, q_cols : q_cols + rot_cols].transpose(1, 0, 2).reshape(seq_count, -1)
    latent_raw = packed[:, :, q_cols + rot_cols :].transpose(1, 0, 2).reshape(seq_count, -1)
    heads_all = rot_mine.shape[1] // rope_width
    own_normed = lax.dynamic_slice_in_dim(normed, tp_rank * seq_count, seq_count, 0)
    rope_raw = jnp.dot(own_normed, w_rope_down, preferred_element_type=jnp.float32).astype(
        jnp.bfloat16
    )
    new_latent = rms_scale(latent_raw, latent_gain).astype(jnp.bfloat16)
    position = lengths.astype(jnp.float32)
    new_rope = rotate(rope_raw.astype(jnp.float32), position).astype(jnp.bfloat16)
    q_pe = rotate(
        rot_mine.reshape(seq_count, heads_all, rope_width).astype(jnp.float32), position[:, None]
    )
    q_pe = q_pe.astype(jnp.bfloat16)
    score_scale = (nope_width + rope_width) ** (-0.5)
    attended = attend(
        q_mine.reshape(seq_count, heads_all, -1),
        q_pe,
        cache_latent,
        cache_rope,
        new_latent,
        new_rope,
        lengths,
        score_scale,
    )
    head_latent = lax.all_to_all(
        attended.reshape(seq_count, -1), "tp", split_axis=1, concat_axis=0, tiled=True
    )
    values = (
        jnp.einsum(
            "thc,hcv->thv",
            head_latent.reshape(group_rows, heads_here, -1),
            w_value_up,
            preferred_element_type=jnp.float32,
        )
        .astype(jnp.bfloat16)
        .reshape(group_rows, -1)
    )
    head_term = jnp.dot(values, w_output, preferred_element_type=jnp.float32)
    terms = to_sequences(head_term.astype(jnp.bfloat16), tp_size, seq_count)
    mixed = jnp.sum(terms.astype(jnp.float32), axis=0)
    own_tokens = lax.dynamic_slice_in_dim(tokens, tp_rank * seq_count, seq_count, 0)
    own_resid = (own_tokens.astype(jnp.float32) + rms_scale(mixed, norm_gains[1])).astype(
        jnp.bfloat16
    )
    expert_in = rms_scale(own_resid, norm_gains[2]).astype(jnp.bfloat16)
    everyone = ("ep", "tp")
    devices = lax.axis_size("ep") * tp_size
    copies = jnp.broadcast_to(expert_in[None], (devices,) + expert_in.shape)
    arrived = lax.all_to_all(copies, everyone, split_axis=0, concat_axis=0, tiled=True)
    arrived = arrived.reshape(devices * seq_count, -1)
    gate_sum = jnp.dot(arrived, w_gate[0], preferred_element_type=jnp.float32)
    up_sum = jnp.dot(arrived, w_up[0], preferred_element_type=jnp.float32)
    hidden_units = (jax.nn.silu(gate_sum) * up_sum).astype(jnp.bfloat16)
    pieces = jnp.dot(hidden_units, w_down[0], preferred_element_type=jnp.float32).astype(
        jnp.bfloat16
    )
    pieces = pieces.reshape(devices, seq_count, -1)
    returned = lax.all_to_all(pieces, everyone, split_axis=0, concat_axis=0, tiled=True)
    own_routes = lax.dynamic_slice_in_dim(routes, tp_rank * seq_count, seq_count, 0)
    own_weights = lax.dynamic_slice_in_dim(route_weights, tp_rank * seq_count, seq_count, 0)
    holder = jnp.arange(devices, dtype=jnp.int32) // tp_size
    picks = own_routes[None, :, :] == holder[:, None, None]
    scale = jnp.sum(jnp.where(picks, own_weights[None], 0.0), axis=-1)
    routed = jnp.sum(scale[:, :, None] * returned.astype(jnp.float32), axis=0)
    hidden_out = (own_resid.astype(jnp.float32) + rms_scale(routed, norm_gains[3])).astype(
        jnp.bfloat16
    )
    return (hidden_out, new_latent, new_rope)


LANES = 128
BIG = 20 * 10**9


def lane_chunk(value, index):
    return value[:, index * LANES : (index + 1) * LANES]


def mean_scale(value, count):
    return lax.rsqrt(jnp.sum(value * value, keepdims=True) / count + EPSILON)


def angle_kernel(lengths, table):
    half = LANES // 2
    lane = lax.broadcasted_iota(jnp.int32, (1, LANES), 1)
    exponent = (lane % (half // 2)).astype(jnp.float32) * (-math.log(ROTARY_BASE) / (half // 2))
    angles = lengths[0].astype(jnp.float32) * jnp.exp(exponent)
    sine = jnp.sin(angles)
    table[0:1, :] = jnp.cos(angles)
    table[1:2, :] = jnp.where(lane % half < half // 2, -sine, sine)


def tail_kernel(
    table,
    tokens,
    gains,
    w_query_rope,
    w_latent,
    w_rope,
    normed_rows,
    tail_rows,
    rope_row,
    token_rows,
    gain_rows,
):
    group_rows, width = tokens.shape
    pieces = width // LANES
    heads = w_query_rope.shape[1] * 2 // LANES
    tail = tail_rows.shape[0] // group_rows
    tokens_f = tokens[...].astype(jnp.float32)
    power = jnp.sum(tokens_f * tokens_f, axis=-1, keepdims=True) / width
    normed = (tokens_f * lax.rsqrt(power + EPSILON) * gains[0:1, :]).astype(jnp.bfloat16)
    normed_rows[...] = normed
    q_rot = jnp.dot(normed, w_query_rope[...], preferred_element_type=jnp.float32)
    latent_cols = jnp.dot(normed, w_latent[...], preferred_element_type=jnp.float32)
    rope_raw = lax.dot_general(
        normed, w_rope[...], (((1,), (1,)), ((), ())), preferred_element_type=jnp.float32
    )
    half = LANES // 2
    low = lax.broadcasted_iota(jnp.int32, (group_rows, LANES), 1) < half
    for h in range(heads):
        pair = lane_chunk(q_rot, h // 2)
        turned = pltpu.roll(pair, half, 1)
        twice = jnp.where(low, pair, turned) if h % 2 == 0 else jnp.where(low, turned, pair)
        tail_rows[pl.ds(h, group_rows, stride=tail), :] = twice
    for k in range(heads, tail):
        tail_rows[pl.ds(k, group_rows, stride=tail), :] = latent_cols
    for k in range(pieces):
        token_rows[pl.ds(k, group_rows, stride=pieces), :] = lane_chunk(tokens_f, k)
        gain_rows[pl.ds(k, gains.shape[0], stride=pieces), :] = lane_chunk(gains[...], k)
    mine = lax.broadcasted_iota(jnp.int32, rope_raw.shape, 0) == lax.axis_index("tp")
    rope_raw = jnp.sum(jnp.where(mine, rope_raw, 0.0), axis=0, keepdims=True)
    rope_raw = rope_raw.astype(jnp.bfloat16).astype(jnp.float32)
    twice = jnp.concatenate([rope_raw, rope_raw], axis=1)
    turned = twice * table[0:1, :] + pltpu.roll(twice, half // 2, 1) * table[1:2, :]
    rope_row[...] = turned.astype(jnp.bfloat16).astype(jnp.float32)


def query_kernel(normed, tail_rows, w_query, w_key, send, rows):
    group_rows = normed.shape[0]
    heads, nope, latent = w_key.shape
    per_head = latent // LANES
    base = heads * per_head
    tail = tail_rows.shape[0] // group_rows
    q_nope = jnp.dot(normed[...], w_query[...], preferred_element_type=jnp.float32)
    q_nope = q_nope.astype(jnp.bfloat16)
    for h in range(heads):
        q_latent = jnp.dot(
            q_nope[:, h * nope : (h + 1) * nope], w_key[h], preferred_element_type=jnp.float32
        )
        for k in range(per_head):
            rows[pl.ds(h * per_head + k, group_rows, stride=base), :] = lane_chunk(q_latent, k)
    for j in range(group_rows):
        send[j, :base] = rows[pl.ds(j * base, base), :].astype(jnp.bfloat16)
        send[j, base:] = tail_rows[pl.ds(j * tail, tail), :].astype(jnp.bfloat16)


def attend_kernel(
    length,
    received,
    cache,
    cache_rope,
    table,
    gain,
    rope_row,
    send,
    latent_rows,
    rows,
    extra,
    rot_rows,
    queries,
    score_scale,
):
    sources, block, _ = received.shape
    latent = cache.shape[1]
    per_head = latent // LANES
    rope = cache_rope.shape[0]
    heads = queries.shape[0]
    here = heads // sources
    base = here * per_head
    tail = block - base
    for j in range(sources):
        piece = received[j].astype(jnp.float32)
        rows[pl.ds(j * base, base), :] = piece[:base]
        extra[pl.ds(j * tail, tail), :] = piece[base:]
    for k in range(per_head):
        queries[:, k * LANES : (k + 1) * LANES] = rows[
            pl.ds(k, heads, stride=per_head), :
        ].astype(jnp.bfloat16)
    for j in range(sources):
        rot_rows[pl.ds(j * here, here), :] = extra[pl.ds(j * tail, here), :]
    latent_raw = extra[pl.ds(here, sources, stride=tail), :]
    latent_f = (latent_raw * mean_scale(latent_raw, latent) * gain[...]).astype(jnp.bfloat16)
    latent_f = latent_f.astype(jnp.float32)
    latent_rows[...] = latent_f
    rot = rot_rows[...]
    q_pe = rot * table[0:1, :] + pltpu.roll(rot, LANES // 4, 1) * table[1:2, :]
    q_pe = q_pe[:, :rope].astype(jnp.bfloat16)
    q = queries[...]
    scores = lax.dot_general(
        q, cache[...], (((1,), (1,)), ((), ())), preferred_element_type=jnp.float32
    )
    scores = scores + jnp.dot(q_pe, cache_rope[...], preferred_element_type=jnp.float32)
    scores = scores * score_scale
    q_f = q.astype(jnp.float32)
    products = lane_chunk(q_f, 0) * latent_f[0:1, :]
    for k in range(1, per_head):
        products = products + lane_chunk(q_f, k) * latent_f[k : k + 1, :]
    own = jnp.sum(products, axis=1, keepdims=True)
    own = own + jnp.sum(
        q_pe.astype(jnp.float32) * rope_row[:, :rope], axis=1, keepdims=True
    )
    own = own * score_scale
    visible = lax.broadcasted_iota(jnp.int32, scores.shape, 1) < length[0]
    top = jnp.maximum(jnp.max(jnp.where(visible, scores, -jnp.inf), axis=1, keepdims=True), own)
    weights = jnp.where(visible, jnp.exp(scores - top), 0.0)
    own_weight = jnp.exp(own - top)
    total = jnp.sum(weights, axis=1, keepdims=True) + own_weight
    probs = (weights / total).astype(jnp.bfloat16)
    own_prob = (own_weight / total).astype(jnp.bfloat16).astype(jnp.float32)
    attended = jnp.dot(probs, cache[...], preferred_element_type=jnp.float32)
    for k in range(per_head):
        rows[pl.ds(k, heads, stride=per_head), :] = (
            lane_chunk(attended, k) + own_prob * latent_f[k : k + 1, :]
        )
    for j in range(sources):
        send[j] = rows[pl.ds(j * base, base), :].astype(jnp.bfloat16)


def output_kernel(received, w_value, w_output, send, rows, term_rows):
    sources, block, _ = received.shape
    heads, latent, _ = w_value.shape
    per_head = latent // LANES
    pieces = w_output.shape[1] // LANES
    for j in range(sources):
        rows[pl.ds(j * block, block), :] = received[j].astype(jnp.float32)
    values = []
    for h in range(heads):
        attended = jnp.concatenate(
            [
                rows[pl.ds(h * per_head + k, sources, stride=block), :].astype(jnp.bfloat16)
                for k in range(per_head)
            ],
            axis=1,
        )
        values.append(
            jnp.dot(attended, w_value[h], preferred_element_type=jnp.float32).astype(jnp.bfloat16)
        )
    values = jnp.concatenate(values, axis=1)
    step = 4
    for c in range(0, pieces, step):
        term = jnp.dot(
            values,
            w_output[:, c * LANES : (c + step) * LANES],
            preferred_element_type=jnp.float32,
        )
        for k in range(step):
            term_rows[pl.ds(c + k, sources, stride=pieces), :] = lane_chunk(term, k)
    for j in range(sources):
        send[j] = term_rows[pl.ds(j * pieces, pieces), :].astype(jnp.bfloat16)


def half_rows(core, count):
    return [core * count + i for i in range(count)]


def pair_kernel(keep, got, send):
    for i in range(send.shape[0]):
        total = keep[i].astype(jnp.float32) + got[i].astype(jnp.float32)
        send[i] = total.astype(jnp.bfloat16)


def pair_half_kernel(keep, got, send, half):
    pair_kernel(keep, got, send)
    for i, row in enumerate(half_rows(lax.axis_index("tp") % 2, half.shape[0])):
        half[i] = send[row]


def combine_kernel(*refs):
    full, half, total = refs[:-2], refs[-2], refs[-1]
    for i in range(total.shape[0]):
        value = jnp.zeros(total.shape[1:], jnp.float32)
        for ref in full:
            value = value + ref[i].astype(jnp.float32)
        total[i] = value.astype(jnp.bfloat16)
    for i, row in enumerate(half_rows(1 - lax.axis_index("tp") % 2, half.shape[0])):
        value = half[i].astype(jnp.float32)
        for ref in full:
            value = value + ref[row].astype(jnp.float32)
        total[row] = value.astype(jnp.bfloat16)


def join_kernel(*refs):
    joined = refs[-1]
    place = 0
    for ref in refs[:-1]:
        for i in range(ref.shape[0]):
            joined[place + i] = ref[i]
        place += ref.shape[0]


def row_scales(blocks, count):
    power = [jnp.sum(block * block, axis=0, keepdims=True) for block in blocks]
    power = jnp.sum(jnp.concatenate(power, axis=0), axis=1, keepdims=True) / count
    scale = lax.rsqrt(power + EPSILON)
    return [scale[i : i + 1, :] for i in range(len(blocks))]


def resid_kernel(
    routes,
    route_weights,
    token_rows,
    gain_rows,
    own,
    partial,
    got,
    send,
    half,
    resid,
    scales,
    after_rows,
):
    rank = lax.axis_index("tp")
    mine = lax.broadcasted_iota(jnp.int32, routes.shape, 1) == rank
    named = jnp.sum(jnp.where(mine, routes[...], 0), axis=1, keepdims=True)
    weight = jnp.sum(jnp.where(mine, route_weights[...], 0.0), axis=1, keepdims=True)
    for e in range(scales.shape[0]):
        total = jnp.sum(jnp.where(named == e, weight, 0.0), axis=0, keepdims=True)
        scales[e : e + 1, :] = jnp.broadcast_to(total, (1, LANES))
    count, pieces, _ = send.shape
    width = pieces * LANES
    mixed = [
        own[i].astype(jnp.float32)
        + (partial[i].astype(jnp.float32) + got[i].astype(jnp.float32))
        for i in range(count)
    ]
    gain = gain_rows[pieces : 2 * pieces, :]
    after = [
        (token_rows[i * pieces : (i + 1) * pieces, :] + mixed[i] * scale * gain)
        .astype(jnp.bfloat16)
        .astype(jnp.float32)
        for i, scale in enumerate(row_scales(mixed, width))
    ]
    gain = gain_rows[2 * pieces : 3 * pieces, :]
    for i, scale in enumerate(row_scales(after, width)):
        after_rows[i] = after[i]
        send[i] = (after[i] * scale * gain).astype(jnp.bfloat16)
    resid[...] = after_rows[rank]
    for i, row in enumerate(half_rows(rank % 2, half.shape[0])):
        half[i] = send[row]


def expert_kernel(*refs):
    parts, (w_gate, w_up, w_down, keep, give, rows, inputs) = refs[:-7], refs[-7:]
    blocks = [part[i] for part in parts for i in range(part.shape[0])]
    count = len(blocks)
    pieces = blocks[0].shape[0]
    for i, block in enumerate(blocks):
        rows[pl.ds(i * pieces, pieces), :] = block.astype(jnp.float32)
    for k in range(pieces):
        inputs[:, k * LANES : (k + 1) * LANES] = rows[
            pl.ds(k, count, stride=pieces), :
        ].astype(jnp.bfloat16)
    gate = jnp.dot(inputs[...], w_gate[...], preferred_element_type=jnp.float32)
    up = jnp.dot(inputs[...], w_up[...], preferred_element_type=jnp.float32)
    inner = (gate / (1.0 + jnp.exp(-gate)) * up).astype(jnp.bfloat16)
    step = 4
    for k in range(0, pieces, step):
        piece = jnp.dot(
            inner, w_down[:, k * LANES : (k + step) * LANES], preferred_element_type=jnp.float32
        )
        piece = piece.astype(jnp.bfloat16).astype(jnp.float32)
        for j in range(step):
            rows[pl.ds(k + j, count, stride=pieces), :] = lane_chunk(piece, j)
    core = lax.axis_index("tp") % 2
    half = pieces // 2
    for i in range(count):
        start = pl.multiple_of(i * pieces + core * half, half)
        keep[i] = rows[pl.ds(start, half), :]
        start = pl.multiple_of(i * pieces + (1 - core) * half, half)
        give[i] = rows[pl.ds(start, half), :].astype(jnp.bfloat16)


def place_kernel(own, mine, others, got, send, masks):
    members, joined = own.shape[0], mine.shape[0]
    core = lax.axis_index("tp") % 2
    group = lax.axis_index("ep")
    pairs, last = masks

    def places(side):
        listed = []
        for low, high in pairs:
            other = group ^ jnp.where(side == 0, low, high)
            listed += [other * members + i for i in range(members)]
        return listed + [(group ^ last) * members + row for row in half_rows(side, members // 2)]

    def put(place, kept, other):
        send[place] = (kept + other.astype(jnp.float32)).astype(jnp.bfloat16)

    for i in range(members):
        put(group * members + i, own[i], got[i])
    for i, place in enumerate(places(1 - core)):
        put(place, mine[i], got[members + joined + i])
    for i, place in enumerate(places(core)):
        put(place, others[i], got[members + i])


def final_kernel(
    scales, received, resid, gain_rows, latent_rows, rope_row, hidden, new_latent, new_rope
):
    for k in range(latent_rows.shape[0]):
        new_latent[:, k * LANES : (k + 1) * LANES] = latent_rows[k : k + 1, :].astype(
            jnp.bfloat16
        )
    new_rope[...] = rope_row[:, : new_rope.shape[1]].astype(jnp.bfloat16)
    sources, half, _ = received.shape
    pieces = 2 * half
    experts = scales.shape[0]
    per_expert = sources // experts
    parts = []
    for c in range(2):
        total = None
        for e in range(experts):
            block = received[e * per_expert + c].astype(jnp.float32)
            for b in range(c + 2, per_expert, 2):
                block = block + received[e * per_expert + b].astype(jnp.float32)
            part = block * scales[e : e + 1, :]
            total = part if total is None else total + part
        parts.append(total)
    routed = jnp.concatenate(parts, axis=0)
    out = resid[...] + routed * mean_scale(routed, pieces * LANES) * gain_rows[3 * pieces :]
    for k in range(pieces):
        hidden[:, k * LANES : (k + 1) * LANES] = out[k : k + 1, :].astype(jnp.bfloat16)


def kernel_call(body, outs, specs, scratch, megabytes, flops, name):
    bytes_moved = flops // BIG * 32 * 1024 * 1024 if flops >= BIG else min(flops, 4 * 1024 * 1024)
    return pl.pallas_call(
        body,
        out_shape=outs,
        in_specs=specs,
        out_specs=jax.tree.map(lambda _: pl.BlockSpec(memory_space=pltpu.VMEM), outs),
        scratch_shapes=scratch,
        compiler_params=pltpu.CompilerParams(vmem_limit_bytes=megabytes * 1024 * 1024),
        cost_estimate=pl.CostEstimate(
            flops=flops, bytes_accessed=bytes_moved, transcendentals=0
        ),
        name=name,
    )


def mask_pairs(size):
    return [(m, m - 1) for m in range(size - 1, 1, -2)], 1


def far_half_pairs(size):
    return [(m, m + 1) for m in range(1, size - 1, 2)], size - 1


def power_of_two(size):
    return size & (size - 1) == 0


def lanes_fit(w_key_up, w_value_up, w_latent_down, w_rope_down, cache_latent, tp_size):
    return (
        cache_latent.shape[0] == 1
        and power_of_two(tp_size)
        and power_of_two(lax.axis_size("ep"))
        and tp_size > 2
        and lax.axis_size("ep") > 1
        and w_latent_down.shape[1] == LANES
        and w_key_up.shape[0] % 2 == 0
        and w_key_up.shape[1] == LANES
        and w_value_up.shape[2] == LANES
        and 2 * w_rope_down.shape[1] == LANES
        and w_key_up.shape[2] == tp_size * LANES
        and w_key_up.shape[0] * w_key_up.shape[2] // LANES % 8 == 0
        and w_key_up.shape[0] < 8
    )


def on_device_fused(
    tokens,
    norm_gains,
    w_query,
    w_query_rope,
    w_key_up,
    w_value_up,
    w_output,
    w_latent_down,
    latent_gain,
    w_rope_down,
    cache_latent,
    cache_rope,
    lengths,
    routes,
    route_weights,
    w_gate,
    w_up,
    w_down,
):
    tp_size = lax.axis_size("tp")
    ep_size = lax.axis_size("ep")
    devices = tp_size * ep_size
    heads_here, nope, latent = w_key_up.shape
    heads = heads_here * tp_size
    chips = tp_size // 2
    group_rows, width = tokens.shape
    rope = w_rope_down.shape[1]
    cached = cache_latent.shape[1]
    pieces = width // LANES
    per_head = latent // LANES
    base = heads_here * per_head
    block = base + 8
    bf16, f32 = jnp.bfloat16, jnp.float32
    vmem = pl.BlockSpec(memory_space=pltpu.VMEM)
    smem = pl.BlockSpec(memory_space=pltpu.SMEM)
    shape = jax.ShapeDtypeStruct

    table = kernel_call(
        angle_kernel, shape((2, LANES), f32), [smem], [], 1, 2 * BIG, "angles"
    )(lengths)
    normed, tail_rows, rope_row, token_rows, gain_rows = kernel_call(
        tail_kernel,
        (
            shape((group_rows, width), bf16),
            shape((group_rows * 8, LANES), f32),
            shape((1, LANES), f32),
            shape((group_rows * pieces, LANES), f32),
            shape((norm_gains.shape[0] * pieces, LANES), f32),
        ),
        [vmem] * 6,
        [],
        6,
        1,
        "tails",
    )(table, tokens, norm_gains, w_query_rope, w_latent_down, w_rope_down.T)
    send = kernel_call(
        query_kernel,
        shape((tp_size, block, LANES), bf16),
        [vmem] * 4,
        [pltpu.VMEM((group_rows * base, LANES), f32)],
        6,
        BIG,
        "queries",
    )(normed, tail_rows, w_query, w_key_up)
    received = lax.all_to_all(send, "tp", split_axis=0, concat_axis=0, tiled=True)
    send, latent_rows = kernel_call(
        functools.partial(attend_kernel, score_scale=(nope + rope) ** (-0.5)),
        (shape((tp_size, base, LANES), bf16), shape((per_head, LANES), f32)),
        [smem] + [vmem] * 6,
        [
            pltpu.VMEM((tp_size * base, LANES), f32),
            pltpu.VMEM((tp_size * 8, LANES), f32),
            pltpu.VMEM((heads, LANES), f32),
            pltpu.VMEM((heads, latent), bf16),
        ],
        8,
        4 * heads * cached * latent,
        "attend",
    )(
        lengths,
        received,
        cache_latent[0],
        cache_rope[0].T,
        table,
        latent_gain.reshape(-1, LANES),
        rope_row,
    )
    received = lax.all_to_all(send, "tp", split_axis=0, concat_axis=0, tiled=True)
    everyone = ("ep", "tp")

    def swap(value):
        return lax.ppermute(value, "tp", [(i, i ^ 1) for i in range(tp_size)])

    def plane(value, low, high):
        pairs = [(i, i ^ (2 * (high if i % 2 else low)) ^ 1) for i in range(tp_size)]
        return lax.ppermute(value, "tp", pairs)

    def along(value, low, high):
        pairs = [(i, i ^ (tp_size * (high if i % 2 else low)) ^ 1) for i in range(devices)]
        return lax.ppermute(value, everyone, pairs)

    send = kernel_call(
        output_kernel,
        shape((tp_size, pieces, LANES), bf16),
        [vmem] * 3,
        [
            pltpu.VMEM((tp_size * base, LANES), f32),
            pltpu.VMEM((tp_size * pieces, LANES), f32),
        ],
        10,
        2 * group_rows * (w_output.size + w_value_up.size),
        "outputs",
    )(received, w_value_up, w_output)
    row_block = shape((tp_size, pieces, LANES), bf16)
    half_block = shape((chips, pieces, LANES), bf16)
    own, half = kernel_call(
        pair_half_kernel, (row_block, half_block), [vmem] * 2, [], 2, send.size, "pair_rows"
    )(send, swap(send))
    pairs, last = mask_pairs(chips)
    parts = [plane(own, low, high) for low, high in pairs] + [plane(half, last, last)]
    partial = kernel_call(
        combine_kernel, row_block, [vmem] * len(parts), [], 2, send.size, "combine"
    )(*parts)
    send, half, resid, scales = kernel_call(
        resid_kernel,
        (
            row_block,
            half_block,
            shape((pieces, LANES), f32),
            shape((ep_size, LANES), f32),
        ),
        [vmem] * 7,
        [pltpu.VMEM((tp_size, pieces, LANES), f32)],
        4,
        10 * tp_size * width,
        "resid",
    )(routes.T, route_weights.T, token_rows, gain_rows, own, partial, swap(partial))
    masks = far_half_pairs(ep_size)
    pairs, last = masks
    parts = [along(send, low, high) for low, high in pairs] + [along(half, last, last)]
    joined = len(pairs) * tp_size + chips
    mine = kernel_call(
        join_kernel,
        shape((joined, pieces, LANES), bf16),
        [vmem] * len(parts),
        [],
        2,
        send.size,
        "join",
    )(*parts)
    others = swap(mine)
    half = pieces // 2

    def run_experts(parts, name):
        count = sum(part.shape[0] for part in parts)
        return kernel_call(
            expert_kernel,
            (shape((count, half, LANES), f32), shape((count, half, LANES), bf16)),
            [vmem] * (len(parts) + 3),
            [pltpu.VMEM((count * pieces, LANES), f32), pltpu.VMEM((count, width), bf16)],
            8,
            2 * 10**9,
            name,
        )(*parts, w_gate[0], w_up[0], w_down[0])

    own_keep, own_give = run_experts([send], "experts_own")
    mine_keep, mine_give = run_experts(parts, "experts_mine")
    others_keep, others_give = run_experts([others], "experts_others")
    give = kernel_call(
        join_kernel,
        shape((devices, half, LANES), bf16),
        [vmem] * 3,
        [],
        2,
        send.size,
        "join_pieces",
    )(own_give, mine_give, others_give)
    send = kernel_call(
        functools.partial(place_kernel, masks=masks),
        shape((devices, half, LANES), bf16),
        [vmem] * 4,
        [],
        4,
        send.size,
        "place",
    )(own_keep, mine_keep, others_keep, swap(give))
    received = lax.all_to_all(send, everyone, split_axis=0, concat_axis=0, tiled=True)
    return kernel_call(
        final_kernel,
        (shape((1, width), bf16), shape((1, latent), bf16), shape((1, rope), bf16)),
        [vmem] * 6,
        [],
        4,
        2 * devices * width,
        "final",
    )(scales, received, resid, gain_rows, latent_rows, rope_row)


def on_device(*arrays):
    w_key_up, w_value_up, w_latent_down, w_rope_down = (arrays[i] for i in (4, 5, 7, 9))
    if lanes_fit(
        w_key_up, w_value_up, w_latent_down, w_rope_down, arrays[10], lax.axis_size("tp")
    ):
        return on_device_fused(*arrays)
    return on_device_plain(*arrays)


def solution(mesh):
    in_specs = (
        P("ep", None),
        P(),
        P(None, "tp"),
        P(None, "tp"),
        P("tp", None, None),
        P("tp", None, None),
        P("tp", None),
        P(None, "tp"),
        P(),
        P(),
        P(("ep", "tp"), None, None),
        P(("ep", "tp"), None, None),
        P(("ep", "tp")),
        P("ep", None),
        P("ep", None),
        P("ep", None, "tp"),
        P("ep", None, "tp"),
        P("ep", "tp", None),
    )
    out_specs = (P(("ep", "tp"), None), P(("ep", "tp"), None), P(("ep", "tp"), None))
    return jax.shard_map(
        on_device, mesh=mesh, in_specs=in_specs, out_specs=out_specs, check_vma=False
    )
```

```python
import functools
import math

import jax
import jax.numpy as jnp
from jax import lax
from jax.experimental import pallas as pl
from jax.experimental.pallas import tpu as pltpu
from jax.sharding import PartitionSpec as P

EPSILON = 1e-06
ROTARY_BASE = 500000.0


def rms_scale(source, gain_row):
    values_f = source.astype(jnp.float32)
    return (
        values_f
        * lax.rsqrt(jnp.mean(values_f * values_f, axis=-1, keepdims=True) + EPSILON)
        * gain_row
    )


def rotate(source, position):
    half_width = source.shape[-1] // 2
    frequency = ROTARY_BASE ** (-jnp.arange(half_width, dtype=jnp.float32) / half_width)
    angles = position[..., None] * frequency
    first_half = source[..., :half_width]
    second_half = source[..., half_width:]
    return jnp.concatenate(
        [
            first_half * jnp.cos(angles) - second_half * jnp.sin(angles),
            second_half * jnp.cos(angles) + first_half * jnp.sin(angles),
        ],
        axis=-1,
    )


def attend(q_latent, q_pe, cache_lat, cache_rp, lat_new, rope_new, lengths, score_scale):
    scores = (
        jnp.einsum("shc,spc->shp", q_latent, cache_lat, preferred_element_type=jnp.float32)
        + jnp.einsum("shr,spr->shp", q_pe, cache_rp, preferred_element_type=jnp.float32)
    ) * score_scale
    own_score = (
        jnp.einsum("shc,sc->sh", q_latent, lat_new, preferred_element_type=jnp.float32)
        + jnp.einsum("shr,sr->sh", q_pe, rope_new, preferred_element_type=jnp.float32)
    ) * score_scale
    visible = (
        jnp.arange(cache_lat.shape[1], dtype=jnp.int32)[None, None, :] < lengths[:, None, None]
    )
    row_max = jnp.maximum(jnp.max(jnp.where(visible, scores, -jnp.inf), axis=-1), own_score)
    weights = jnp.where(visible, jnp.exp(scores - row_max[..., None]), 0.0)
    own_weight = jnp.exp(own_score - row_max)
    denominator = jnp.sum(weights, axis=-1) + own_weight
    probabilities = (weights / denominator[..., None]).astype(jnp.bfloat16)
    own_prob = (own_weight / denominator).astype(jnp.bfloat16)
    attended = jnp.einsum(
        "shp,spc->shc", probabilities, cache_lat, preferred_element_type=jnp.float32
    )
    attended = (
        attended + own_prob.astype(jnp.float32)[..., None] * lat_new.astype(jnp.float32)[:, None, :]
    )
    return attended.astype(jnp.bfloat16)


def to_sequences(rows, tp_size, seq_count):
    blocks = rows.reshape(tp_size, seq_count, rows.shape[1])
    return lax.all_to_all(blocks, "tp", split_axis=0, concat_axis=0, tiled=True)


def on_device_plain(
    tokens,
    norm_gains,
    w_query,
    w_query_rope,
    w_key_up,
    w_value_up,
    w_output,
    w_latent_down,
    latent_gain,
    w_rope_down,
    cache_latent,
    cache_rope,
    lengths,
    routes,
    route_weights,
    w_gate,
    w_up,
    w_down,
):
    group_rows = tokens.shape[0]
    seq_count = cache_latent.shape[0]
    heads_here = w_key_up.shape[0]
    nope_width = w_key_up.shape[1]
    rope_width = w_rope_down.shape[1]
    tp_size = lax.axis_size("tp")
    tp_rank = lax.axis_index("tp")
    normed = rms_scale(tokens, norm_gains[0]).astype(jnp.bfloat16)
    q_nope = jnp.dot(normed, w_query, preferred_element_type=jnp.float32).astype(jnp.bfloat16)
    q_nope = q_nope.reshape(group_rows, heads_here, nope_width)
    q_latent = jnp.einsum("thn,hnc->thc", q_nope, w_key_up, preferred_element_type=jnp.float32)
    q_latent = q_latent.astype(jnp.bfloat16).reshape(group_rows, -1)
    q_rot = jnp.dot(normed, w_query_rope, preferred_element_type=jnp.float32).astype(jnp.bfloat16)
    latent_cols = jnp.dot(normed, w_latent_down, preferred_element_type=jnp.float32).astype(
        jnp.bfloat16
    )
    q_cols, rot_cols = q_latent.shape[1], q_rot.shape[1]
    packed = jnp.concatenate([q_latent, q_rot, latent_cols], axis=1)
    packed = to_sequences(packed, tp_size, seq_count)
    q_mine = packed[:, :, :q_cols].transpose(1, 0, 2).reshape(seq_count, -1)
    rot_mine = packed[:, :, q_cols : q_cols + rot_cols].transpose(1, 0, 2).reshape(seq_count, -1)
    latent_raw = packed[:, :, q_cols + rot_cols :].transpose(1, 0, 2).reshape(seq_count, -1)
    heads_all = rot_mine.shape[1] // rope_width
    own_normed = lax.dynamic_slice_in_dim(normed, tp_rank * seq_count, seq_count, 0)
    rope_raw = jnp.dot(own_normed, w_rope_down, preferred_element_type=jnp.float32).astype(
        jnp.bfloat16
    )
    new_latent = rms_scale(latent_raw, latent_gain).astype(jnp.bfloat16)
    position = lengths.astype(jnp.float32)
    new_rope = rotate(rope_raw.astype(jnp.float32), position).astype(jnp.bfloat16)
    q_pe = rotate(
        rot_mine.reshape(seq_count, heads_all, rope_width).astype(jnp.float32), position[:, None]
    )
    q_pe = q_pe.astype(jnp.bfloat16)
    score_scale = (nope_width + rope_width) ** (-0.5)
    attended = attend(
        q_mine.reshape(seq_count, heads_all, -1),
        q_pe,
        cache_latent,
        cache_rope,
        new_latent,
        new_rope,
        lengths,
        score_scale,
    )
    head_latent = lax.all_to_all(
        attended.reshape(seq_count, -1), "tp", split_axis=1, concat_axis=0, tiled=True
    )
    values = (
        jnp.einsum(
            "thc,hcv->thv",
            head_latent.reshape(group_rows, heads_here, -1),
            w_value_up,
            preferred_element_type=jnp.float32,
        )
        .astype(jnp.bfloat16)
        .reshape(group_rows, -1)
    )
    head_term = jnp.dot(values, w_output, preferred_element_type=jnp.float32)
    terms = to_sequences(head_term.astype(jnp.bfloat16), tp_size, seq_count)
    mixed = jnp.sum(terms.astype(jnp.float32), axis=0)
    own_tokens = lax.dynamic_slice_in_dim(tokens, tp_rank * seq_count, seq_count, 0)
    own_resid = (own_tokens.astype(jnp.float32) + rms_scale(mixed, norm_gains[1])).astype(
        jnp.bfloat16
    )
    expert_in = rms_scale(own_resid, norm_gains[2]).astype(jnp.bfloat16)
    everyone = ("ep", "tp")
    devices = lax.axis_size("ep") * tp_size
    copies = jnp.broadcast_to(expert_in[None], (devices,) + expert_in.shape)
    arrived = lax.all_to_all(copies, everyone, split_axis=0, concat_axis=0, tiled=True)
    arrived = arrived.reshape(devices * seq_count, -1)
    gate_sum = jnp.dot(arrived, w_gate[0], preferred_element_type=jnp.float32)
    up_sum = jnp.dot(arrived, w_up[0], preferred_element_type=jnp.float32)
    hidden_units = (jax.nn.silu(gate_sum) * up_sum).astype(jnp.bfloat16)
    pieces = jnp.dot(hidden_units, w_down[0], preferred_element_type=jnp.float32).astype(
        jnp.bfloat16
    )
    pieces = pieces.reshape(devices, seq_count, -1)
    returned = lax.all_to_all(pieces, everyone, split_axis=0, concat_axis=0, tiled=True)
    own_routes = lax.dynamic_slice_in_dim(routes, tp_rank * seq_count, seq_count, 0)
    own_weights = lax.dynamic_slice_in_dim(route_weights, tp_rank * seq_count, seq_count, 0)
    holder = jnp.arange(devices, dtype=jnp.int32) // tp_size
    picks = own_routes[None, :, :] == holder[:, None, None]
    scale = jnp.sum(jnp.where(picks, own_weights[None], 0.0), axis=-1)
    routed = jnp.sum(scale[:, :, None] * returned.astype(jnp.float32), axis=0)
    hidden_out = (own_resid.astype(jnp.float32) + rms_scale(routed, norm_gains[3])).astype(
        jnp.bfloat16
    )
    return (hidden_out, new_latent, new_rope)


LANES = 128
BIG = 20 * 10**9


def lane_chunk(value, index):
    return value[:, index * LANES : (index + 1) * LANES]


def mean_scale(value, count):
    return lax.rsqrt(jnp.sum(value * value, keepdims=True) / count + EPSILON)


def angle_kernel(lengths, table):
    half = LANES // 2
    lane = lax.broadcasted_iota(jnp.int32, (1, LANES), 1)
    exponent = (lane % (half // 2)).astype(jnp.float32) * (-math.log(ROTARY_BASE) / (half // 2))
    angles = lengths[0].astype(jnp.float32) * jnp.exp(exponent)
    sine = jnp.sin(angles)
    table[0:1, :] = jnp.cos(angles)
    table[1:2, :] = jnp.where(lane % half < half // 2, -sine, sine)


def tail_kernel(
    table,
    tokens,
    gains,
    w_query_rope,
    w_latent,
    w_rope,
    normed_rows,
    tail_rows,
    rope_row,
    token_rows,
    gain_rows,
):
    group_rows, width = tokens.shape
    pieces = width // LANES
    heads = w_query_rope.shape[1] * 2 // LANES
    tail = tail_rows.shape[0] // group_rows
    tokens_f = tokens[...].astype(jnp.float32)
    power = jnp.sum(tokens_f * tokens_f, axis=-1, keepdims=True) / width
    normed = (tokens_f * lax.rsqrt(power + EPSILON) * gains[0:1, :]).astype(jnp.bfloat16)
    normed_rows[...] = normed
    q_rot = jnp.dot(normed, w_query_rope[...], preferred_element_type=jnp.float32)
    latent_cols = jnp.dot(normed, w_latent[...], preferred_element_type=jnp.float32)
    rope_raw = lax.dot_general(
        normed, w_rope[...], (((1,), (1,)), ((), ())), preferred_element_type=jnp.float32
    )
    half = LANES // 2
    low = lax.broadcasted_iota(jnp.int32, (group_rows, LANES), 1) < half
    for h in range(heads):
        pair = lane_chunk(q_rot, h // 2)
        turned = pltpu.roll(pair, half, 1)
        twice = jnp.where(low, pair, turned) if h % 2 == 0 else jnp.where(low, turned, pair)
        tail_rows[pl.ds(h, group_rows, stride=tail), :] = twice
    for k in range(heads, tail):
        tail_rows[pl.ds(k, group_rows, stride=tail), :] = latent_cols
    for k in range(pieces):
        token_rows[pl.ds(k, group_rows, stride=pieces), :] = lane_chunk(tokens_f, k)
        gain_rows[pl.ds(k, gains.shape[0], stride=pieces), :] = lane_chunk(gains[...], k)
    mine = lax.broadcasted_iota(jnp.int32, rope_raw.shape, 0) == lax.axis_index("tp")
    rope_raw = jnp.sum(jnp.where(mine, rope_raw, 0.0), axis=0, keepdims=True)
    rope_raw = rope_raw.astype(jnp.bfloat16).astype(jnp.float32)
    twice = jnp.concatenate([rope_raw, rope_raw], axis=1)
    turned = twice * table[0:1, :] + pltpu.roll(twice, half // 2, 1) * table[1:2, :]
    rope_row[...] = turned.astype(jnp.bfloat16).astype(jnp.float32)


def query_kernel(normed, tail_rows, w_query, w_key, send, rows):
    group_rows = normed.shape[0]
    heads, nope, latent = w_key.shape
    per_head = latent // LANES
    base = heads * per_head
    tail = tail_rows.shape[0] // group_rows
    q_nope = jnp.dot(normed[...], w_query[...], preferred_element_type=jnp.float32)
    q_nope = q_nope.astype(jnp.bfloat16)
    for h in range(heads):
        q_latent = jnp.dot(
            q_nope[:, h * nope : (h + 1) * nope], w_key[h], preferred_element_type=jnp.float32
        )
        for k in range(per_head):
            rows[pl.ds(h * per_head + k, group_rows, stride=base), :] = lane_chunk(q_latent, k)
    for j in range(group_rows):
        send[j, :base] = rows[pl.ds(j * base, base), :].astype(jnp.bfloat16)
        send[j, base:] = tail_rows[pl.ds(j * tail, tail), :].astype(jnp.bfloat16)


def attend_kernel(
    length,
    received,
    cache,
    cache_rope,
    table,
    gain,
    rope_row,
    send,
    latent_rows,
    rows,
    extra,
    rot_rows,
    queries,
    score_scale,
):
    sources, block, _ = received.shape
    latent = cache.shape[1]
    per_head = latent // LANES
    rope = cache_rope.shape[0]
    heads = queries.shape[0]
    here = heads // sources
    base = here * per_head
    tail = block - base
    for j in range(sources):
        piece = received[j].astype(jnp.float32)
        rows[pl.ds(j * base, base), :] = piece[:base]
        extra[pl.ds(j * tail, tail), :] = piece[base:]
    for k in range(per_head):
        queries[:, k * LANES : (k + 1) * LANES] = rows[
            pl.ds(k, heads, stride=per_head), :
        ].astype(jnp.bfloat16)
    for j in range(sources):
        rot_rows[pl.ds(j * here, here), :] = extra[pl.ds(j * tail, here), :]
    latent_raw = extra[pl.ds(here, sources, stride=tail), :]
    latent_f = (latent_raw * mean_scale(latent_raw, latent) * gain[...]).astype(jnp.bfloat16)
    latent_f = latent_f.astype(jnp.float32)
    latent_rows[...] = latent_f
    rot = rot_rows[...]
    q_pe = rot * table[0:1, :] + pltpu.roll(rot, LANES // 4, 1) * table[1:2, :]
    q_pe = q_pe[:, :rope].astype(jnp.bfloat16)
    q = queries[...]
    scores = lax.dot_general(
        q, cache[...], (((1,), (1,)), ((), ())), preferred_element_type=jnp.float32
    )
    scores = scores + jnp.dot(q_pe, cache_rope[...], preferred_element_type=jnp.float32)
    scores = scores * score_scale
    q_f = q.astype(jnp.float32)
    products = lane_chunk(q_f, 0) * latent_f[0:1, :]
    for k in range(1, per_head):
        products = products + lane_chunk(q_f, k) * latent_f[k : k + 1, :]
    own = jnp.sum(products, axis=1, keepdims=True)
    own = own + jnp.sum(
        q_pe.astype(jnp.float32) * rope_row[:, :rope], axis=1, keepdims=True
    )
    own = own * score_scale
    visible = lax.broadcasted_iota(jnp.int32, scores.shape, 1) < length[0]
    top = jnp.maximum(jnp.max(jnp.where(visible, scores, -jnp.inf), axis=1, keepdims=True), own)
    weights = jnp.where(visible, jnp.exp(scores - top), 0.0)
    own_weight = jnp.exp(own - top)
    total = jnp.sum(weights, axis=1, keepdims=True) + own_weight
    probs = (weights / total).astype(jnp.bfloat16)
    own_prob = (own_weight / total).astype(jnp.bfloat16).astype(jnp.float32)
    attended = jnp.dot(probs, cache[...], preferred_element_type=jnp.float32)
    for k in range(per_head):
        rows[pl.ds(k, heads, stride=per_head), :] = (
            lane_chunk(attended, k) + own_prob * latent_f[k : k + 1, :]
        )
    for j in range(sources):
        send[j] = rows[pl.ds(j * base, base), :].astype(jnp.bfloat16)


def output_kernel(received, w_value, w_output, send, rows, term_rows):
    sources, block, _ = received.shape
    heads, latent, _ = w_value.shape
    per_head = latent // LANES
    pieces = w_output.shape[1] // LANES
    for j in range(sources):
        rows[pl.ds(j * block, block), :] = received[j].astype(jnp.float32)
    values = []
    for h in range(heads):
        attended = jnp.concatenate(
            [
                rows[pl.ds(h * per_head + k, sources, stride=block), :].astype(jnp.bfloat16)
                for k in range(per_head)
            ],
            axis=1,
        )
        values.append(
            jnp.dot(attended, w_value[h], preferred_element_type=jnp.float32).astype(jnp.bfloat16)
        )
    values = jnp.concatenate(values, axis=1)
    step = 4
    for c in range(0, pieces, step):
        term = jnp.dot(
            values,
            w_output[:, c * LANES : (c + step) * LANES],
            preferred_element_type=jnp.float32,
        )
        for k in range(step):
            term_rows[pl.ds(c + k, sources, stride=pieces), :] = lane_chunk(term, k)
    for j in range(sources):
        send[j] = term_rows[pl.ds(j * pieces, pieces), :].astype(jnp.bfloat16)


def half_rows(core, count):
    return [core * count + i for i in range(count)]


def pair_kernel(keep, got, send):
    for i in range(send.shape[0]):
        total = keep[i].astype(jnp.float32) + got[i].astype(jnp.float32)
        send[i] = total.astype(jnp.bfloat16)


def pair_half_kernel(keep, got, send, half):
    pair_kernel(keep, got, send)
    for i, row in enumerate(half_rows(lax.axis_index("tp") % 2, half.shape[0])):
        half[i] = send[row]


def combine_kernel(*refs):
    full, half, total = refs[:-2], refs[-2], refs[-1]
    for i in range(total.shape[0]):
        value = jnp.zeros(total.shape[1:], jnp.float32)
        for ref in full:
            value = value + ref[i].astype(jnp.float32)
        total[i] = value.astype(jnp.bfloat16)
    for i, row in enumerate(half_rows(1 - lax.axis_index("tp") % 2, half.shape[0])):
        value = half[i].astype(jnp.float32)
        for ref in full:
            value = value + ref[row].astype(jnp.float32)
        total[row] = value.astype(jnp.bfloat16)


def join_kernel(*refs):
    joined = refs[-1]
    place = 0
    for ref in refs[:-1]:
        for i in range(ref.shape[0]):
            joined[place + i] = ref[i]
        place += ref.shape[0]


def row_scales(blocks, count):
    power = [jnp.sum(block * block, axis=0, keepdims=True) for block in blocks]
    power = jnp.sum(jnp.concatenate(power, axis=0), axis=1, keepdims=True) / count
    scale = lax.rsqrt(power + EPSILON)
    return [scale[i : i + 1, :] for i in range(len(blocks))]


def resid_kernel(
    routes,
    route_weights,
    token_rows,
    gain_rows,
    own,
    partial,
    got,
    send,
    half,
    resid,
    scales,
    after_rows,
):
    rank = lax.axis_index("tp")
    mine = lax.broadcasted_iota(jnp.int32, routes.shape, 1) == rank
    named = jnp.sum(jnp.where(mine, routes[...], 0), axis=1, keepdims=True)
    weight = jnp.sum(jnp.where(mine, route_weights[...], 0.0), axis=1, keepdims=True)
    for e in range(scales.shape[0]):
        total = jnp.sum(jnp.where(named == e, weight, 0.0), axis=0, keepdims=True)
        scales[e : e + 1, :] = jnp.broadcast_to(total, (1, LANES))
    count, pieces, _ = send.shape
    width = pieces * LANES
    mixed = [
        own[i].astype(jnp.float32)
        + (partial[i].astype(jnp.float32) + got[i].astype(jnp.float32))
        for i in range(count)
    ]
    gain = gain_rows[pieces : 2 * pieces, :]
    after = [
        (token_rows[i * pieces : (i + 1) * pieces, :] + mixed[i] * scale * gain)
        .astype(jnp.bfloat16)
        .astype(jnp.float32)
        for i, scale in enumerate(row_scales(mixed, width))
    ]
    gain = gain_rows[2 * pieces : 3 * pieces, :]
    for i, scale in enumerate(row_scales(after, width)):
        after_rows[i] = after[i]
        send[i] = (after[i] * scale * gain).astype(jnp.bfloat16)
    resid[...] = after_rows[rank]
    for i, row in enumerate(half_rows(rank % 2, half.shape[0])):
        half[i] = send[row]


def expert_kernel(*refs):
    parts, (w_gate, w_up, w_down, keep, give, rows, inputs) = refs[:-7], refs[-7:]
    blocks = [part[i] for part in parts for i in range(part.shape[0])]
    count = len(blocks)
    pieces = blocks[0].shape[0]
    for i, block in enumerate(blocks):
        rows[pl.ds(i * pieces, pieces), :] = block.astype(jnp.float32)
    for k in range(pieces):
        inputs[:, k * LANES : (k + 1) * LANES] = rows[
            pl.ds(k, count, stride=pieces), :
        ].astype(jnp.bfloat16)
    gate = jnp.dot(inputs[...], w_gate[...], preferred_element_type=jnp.float32)
    up = jnp.dot(inputs[...], w_up[...], preferred_element_type=jnp.float32)
    inner = (gate / (1.0 + jnp.exp(-gate)) * up).astype(jnp.bfloat16)
    step = 4
    for k in range(0, pieces, step):
        piece = jnp.dot(
            inner, w_down[:, k * LANES : (k + step) * LANES], preferred_element_type=jnp.float32
        )
        piece = piece.astype(jnp.bfloat16).astype(jnp.float32)
        for j in range(step):
            rows[pl.ds(k + j, count, stride=pieces), :] = lane_chunk(piece, j)
    core = lax.axis_index("tp") % 2
    half = pieces // 2
    for i in range(count):
        start = pl.multiple_of(i * pieces + core * half, half)
        keep[i] = rows[pl.ds(start, half), :]
        start = pl.multiple_of(i * pieces + (1 - core) * half, half)
        give[i] = rows[pl.ds(start, half), :].astype(jnp.bfloat16)


def place_kernel(own, mine, others, got, send, masks):
    members, joined = own.shape[0], mine.shape[0]
    core = lax.axis_index("tp") % 2
    group = lax.axis_index("ep")
    pairs, last = masks

    def places(side):
        listed = []
        for low, high in pairs:
            other = group ^ jnp.where(side == 0, low, high)
            listed += [other * members + i for i in range(members)]
        return listed + [(group ^ last) * members + row for row in half_rows(side, members // 2)]

    def put(place, kept, other):
        send[place] = (kept + other.astype(jnp.float32)).astype(jnp.bfloat16)

    for i in range(members):
        put(group * members + i, own[i], got[i])
    for i, place in enumerate(places(1 - core)):
        put(place, mine[i], got[members + joined + i])
    for i, place in enumerate(places(core)):
        put(place, others[i], got[members + i])


def final_kernel(
    scales, received, resid, gain_rows, latent_rows, rope_row, hidden, new_latent, new_rope
):
    for k in range(latent_rows.shape[0]):
        new_latent[:, k * LANES : (k + 1) * LANES] = latent_rows[k : k + 1, :].astype(
            jnp.bfloat16
        )
    new_rope[...] = rope_row[:, : new_rope.shape[1]].astype(jnp.bfloat16)
    sources, half, _ = received.shape
    pieces = 2 * half
    experts = scales.shape[0]
    per_expert = sources // experts
    parts = []
    for c in range(2):
        total = None
        for e in range(experts):
            block = received[e * per_expert + c].astype(jnp.float32)
            for b in range(c + 2, per_expert, 2):
                block = block + received[e * per_expert + b].astype(jnp.float32)
            part = block * scales[e : e + 1, :]
            total = part if total is None else total + part
        parts.append(total)
    routed = jnp.concatenate(parts, axis=0)
    out = resid[...] + routed * mean_scale(routed, pieces * LANES) * gain_rows[3 * pieces :]
    for k in range(pieces):
        hidden[:, k * LANES : (k + 1) * LANES] = out[k : k + 1, :].astype(jnp.bfloat16)


def kernel_call(body, outs, specs, scratch, megabytes, flops, name):
    bytes_moved = flops // BIG * 32 * 1024 * 1024 if flops >= BIG else min(flops, 4 * 1024 * 1024)
    return pl.pallas_call(
        body,
        out_shape=outs,
        in_specs=specs,
        out_specs=jax.tree.map(lambda _: pl.BlockSpec(memory_space=pltpu.VMEM), outs),
        scratch_shapes=scratch,
        compiler_params=pltpu.CompilerParams(vmem_limit_bytes=megabytes * 1024 * 1024),
        cost_estimate=pl.CostEstimate(
            flops=flops, bytes_accessed=bytes_moved, transcendentals=0
        ),
        name=name,
    )


def mask_pairs(size):
    return [(m, m - 1) for m in range(size - 1, 1, -2)], 1


def far_half_pairs(size):
    return [(m, m + 1) for m in range(1, size - 1, 2)], size - 1


def power_of_two(size):
    return size & (size - 1) == 0


def lanes_fit(w_key_up, w_value_up, w_latent_down, w_rope_down, cache_latent, tp_size):
    return (
        cache_latent.shape[0] == 1
        and power_of_two(tp_size)
        and power_of_two(lax.axis_size("ep"))
        and tp_size > 2
        and lax.axis_size("ep") > 1
        and w_latent_down.shape[1] == LANES
        and w_key_up.shape[0] % 2 == 0
        and w_key_up.shape[1] == LANES
        and w_value_up.shape[2] == LANES
        and 2 * w_rope_down.shape[1] == LANES
        and w_key_up.shape[2] == tp_size * LANES
        and w_key_up.shape[0] * w_key_up.shape[2] // LANES % 8 == 0
        and w_key_up.shape[0] < 8
    )


def on_device_fused(
    tokens,
    norm_gains,
    w_query,
    w_query_rope,
    w_key_up,
    w_value_up,
    w_output,
    w_latent_down,
    latent_gain,
    w_rope_down,
    cache_latent,
    cache_rope,
    lengths,
    routes,
    route_weights,
    w_gate,
    w_up,
    w_down,
):
    tp_size = lax.axis_size("tp")
    ep_size = lax.axis_size("ep")
    devices = tp_size * ep_size
    heads_here, nope, latent = w_key_up.shape
    heads = heads_here * tp_size
    chips = tp_size // 2
    group_rows, width = tokens.shape
    rope = w_rope_down.shape[1]
    cached = cache_latent.shape[1]
    pieces = width // LANES
    per_head = latent // LANES
    base = heads_here * per_head
    block = base + 8
    bf16, f32 = jnp.bfloat16, jnp.float32
    vmem = pl.BlockSpec(memory_space=pltpu.VMEM)
    smem = pl.BlockSpec(memory_space=pltpu.SMEM)
    shape = jax.ShapeDtypeStruct

    table = kernel_call(
        angle_kernel, shape((2, LANES), f32), [smem], [], 1, 2 * BIG, "angles"
    )(lengths)
    normed, tail_rows, rope_row, token_rows, gain_rows = kernel_call(
        tail_kernel,
        (
            shape((group_rows, width), bf16),
            shape((group_rows * 8, LANES), f32),
            shape((1, LANES), f32),
            shape((group_rows * pieces, LANES), f32),
            shape((norm_gains.shape[0] * pieces, LANES), f32),
        ),
        [vmem] * 6,
        [],
        6,
        1,
        "tails",
    )(table, tokens, norm_gains, w_query_rope, w_latent_down, w_rope_down.T)
    send = kernel_call(
        query_kernel,
        shape((tp_size, block, LANES), bf16),
        [vmem] * 4,
        [pltpu.VMEM((group_rows * base, LANES), f32)],
        6,
        BIG,
        "queries",
    )(normed, tail_rows, w_query, w_key_up)
    received = lax.all_to_all(send, "tp", split_axis=0, concat_axis=0, tiled=True)
    send, latent_rows = kernel_call(
        functools.partial(attend_kernel, score_scale=(nope + rope) ** (-0.5)),
        (shape((tp_size, base, LANES), bf16), shape((per_head, LANES), f32)),
        [smem] + [vmem] * 6,
        [
            pltpu.VMEM((tp_size * base, LANES), f32),
            pltpu.VMEM((tp_size * 8, LANES), f32),
            pltpu.VMEM((heads, LANES), f32),
            pltpu.VMEM((heads, latent), bf16),
        ],
        8,
        4 * heads * cached * latent,
        "attend",
    )(
        lengths,
        received,
        cache_latent[0],
        cache_rope[0].T,
        table,
        latent_gain.reshape(-1, LANES),
        rope_row,
    )
    received = lax.all_to_all(send, "tp", split_axis=0, concat_axis=0, tiled=True)
    everyone = ("ep", "tp")

    def swap(value):
        return lax.ppermute(value, "tp", [(i, i ^ 1) for i in range(tp_size)])

    def plane(value, low, high):
        pairs = [(i, i ^ (2 * (high if i % 2 else low)) ^ 1) for i in range(tp_size)]
        return lax.ppermute(value, "tp", pairs)

    def along(value, low, high):
        pairs = [(i, i ^ (tp_size * (high if i % 2 else low)) ^ 1) for i in range(devices)]
        return lax.ppermute(value, everyone, pairs)

    send = kernel_call(
        output_kernel,
        shape((tp_size, pieces, LANES), bf16),
        [vmem] * 3,
        [
            pltpu.VMEM((tp_size * base, LANES), f32),
            pltpu.VMEM((tp_size * pieces, LANES), f32),
        ],
        10,
        2 * group_rows * (w_output.size + w_value_up.size),
        "outputs",
    )(received, w_value_up, w_output)
    row_block = shape((tp_size, pieces, LANES), bf16)
    half_block = shape((chips, pieces, LANES), bf16)
    own, half = kernel_call(
        pair_half_kernel, (row_block, half_block), [vmem] * 2, [], 2, send.size, "pair_rows"
    )(send, swap(send))
    pairs, last = far_half_pairs(chips)
    parts = [plane(own, low, high) for low, high in pairs] + [plane(half, last, last)]
    partial = kernel_call(
        combine_kernel, row_block, [vmem] * len(parts), [], 2, send.size, "combine"
    )(*parts)
    send, half, resid, scales = kernel_call(
        resid_kernel,
        (
            row_block,
            half_block,
            shape((pieces, LANES), f32),
            shape((ep_size, LANES), f32),
        ),
        [vmem] * 7,
        [pltpu.VMEM((tp_size, pieces, LANES), f32)],
        4,
        10 * tp_size * width,
        "resid",
    )(routes.T, route_weights.T, token_rows, gain_rows, own, partial, swap(partial))
    masks = far_half_pairs(ep_size)
    pairs, last = masks
    parts = [along(send, low, high) for low, high in pairs] + [along(half, last, last)]
    joined = len(pairs) * tp_size + chips
    mine = kernel_call(
        join_kernel,
        shape((joined, pieces, LANES), bf16),
        [vmem] * len(parts),
        [],
        2,
        send.size,
        "join",
    )(*parts)
    others = swap(mine)
    half = pieces // 2

    def run_experts(parts, name):
        count = sum(part.shape[0] for part in parts)
        return kernel_call(
            expert_kernel,
            (shape((count, half, LANES), f32), shape((count, half, LANES), bf16)),
            [vmem] * (len(parts) + 3),
            [pltpu.VMEM((count * pieces, LANES), f32), pltpu.VMEM((count, width), bf16)],
            8,
            2 * 10**9,
            name,
        )(*parts, w_gate[0], w_up[0], w_down[0])

    own_keep, own_give = run_experts([send], "experts_own")
    mine_keep, mine_give = run_experts(parts, "experts_mine")
    others_keep, others_give = run_experts([others], "experts_others")
    give = kernel_call(
        join_kernel,
        shape((devices, half, LANES), bf16),
        [vmem] * 3,
        [],
        2,
        send.size,
        "join_pieces",
    )(own_give, mine_give, others_give)
    send = kernel_call(
        functools.partial(place_kernel, masks=masks),
        shape((devices, half, LANES), bf16),
        [vmem] * 4,
        [],
        4,
        send.size,
        "place",
    )(own_keep, mine_keep, others_keep, swap(give))
    received = lax.all_to_all(send, everyone, split_axis=0, concat_axis=0, tiled=True)
    return kernel_call(
        final_kernel,
        (shape((1, width), bf16), shape((1, latent), bf16), shape((1, rope), bf16)),
        [vmem] * 6,
        [],
        4,
        2 * devices * width,
        "final",
    )(scales, received, resid, gain_rows, latent_rows, rope_row)


def on_device(*arrays):
    w_key_up, w_value_up, w_latent_down, w_rope_down = (arrays[i] for i in (4, 5, 7, 9))
    if lanes_fit(
        w_key_up, w_value_up, w_latent_down, w_rope_down, arrays[10], lax.axis_size("tp")
    ):
        return on_device_fused(*arrays)
    return on_device_plain(*arrays)


def solution(mesh):
    in_specs = (
        P("ep", None),
        P(),
        P(None, "tp"),
        P(None, "tp"),
        P("tp", None, None),
        P("tp", None, None),
        P("tp", None),
        P(None, "tp"),
        P(),
        P(),
        P(("ep", "tp"), None, None),
        P(("ep", "tp"), None, None),
        P(("ep", "tp")),
        P("ep", None),
        P("ep", None),
        P("ep", None, "tp"),
        P("ep", None, "tp"),
        P("ep", "tp", None),
    )
    out_specs = (P(("ep", "tp"), None), P(("ep", "tp"), None), P(("ep", "tp"), None))
    return jax.shard_map(
        on_device, mesh=mesh, in_specs=in_specs, out_specs=out_specs, check_vma=False
    )
```
